512 devices in a mesh: sp: 32 (over z, core), tp: 16 (over y, x).
Axes of the slice: x: 4, y: 4, z: 16, core: 2. Of those that a mesh axis runs over, the one named last changes fastest.
Arguments:
- b_gate: bfloat16 [8192, 1024], P('sp', 'tp'), may hold values from -6 to 6
- c_gate: bfloat16 [8192, 1024], P('sp', 'tp'), may hold values from -6 to 6
- h_in: bfloat16 [8192, 1024], P('sp', 'tp'), may hold values from -6 to 6
- docs: int32 [8192], replicated, may hold values from 0 to 15, never falling along the last dimension, each value on 1 to 1024 neighbouring positions
- conv_taps: bfloat16 [3, 1024], replicated, may hold values from -3 to 3
- out_weight: bfloat16 [1024, 4096], P(None, 'tp'), may hold values from -0.1875 to 0.1875
- residual_in: bfloat16 [8192, 4096], P('sp', 'tp'), may hold values from -52 to 52
- norm_gain: bfloat16 [4096], replicated, may hold values from 0.099609375 to 1.8984375
- expert_pick: int32 [8192, 2], P('sp'), may hold values from 0 to 31, as said below
- route_weight: float32 [8192, 2], P('sp'), may hold values from 0.5 to 2
- w_gate: bfloat16 [32, 4096, 2048], P('sp', None, 'tp'), may hold values from -0.09375 to 0.09375
- w_up: bfloat16 [32, 4096, 2048], P('sp', None, 'tp'), may hold values from -0.09375 to 0.09375
- w_down: bfloat16 [32, 2048, 4096], P('sp', None, 'tp'), may hold values from -0.125 to 0.125
Outputs:
- stream_out: bfloat16 [8192, 4096], P('sp', 'tp')
The draws below stay inside these ranges and needn't reach their ends.
Inputs may be any that keep to these rules, and one draw needn't show every extreme that they name: `expert_pick`: each row names 2 different experts of one group; group g holds experts g * 8 up to the next group's first.
All inputs are finite; a program needn't handle non-finite values.
Results may differ from the reference program's by a relative error of at most 0.012.
Values may be sent and summed in bfloat16 or wider, within the bound.
No kernel may reach another device: no remote copies, remote signals or barrier semaphores. Data moves between devices by JAX's collectives and lax.ppermute only.
A program may use at most 64 MiB of HBM per device.

```python
import math
import jax
import jax.numpy as jnp
import numpy as np
from jax import lax

D = 4096
CH = 1024
FFE = 2048
GROUPS = 4
TOP_K = 2
TOK_DEV = 256
TOKENS = 8192
EXPERTS = 32
CAP = 20
N_SP = 32


def draw_expert_pick(key, part):
    per_group = EXPERTS // GROUPS
    key_group, key_first, key_second = jax.random.split(jax.random.fold_in(key, 11), 3)
    group_ids = jax.random.randint(key_group, (TOKENS,), 0, GROUPS)
    first_pick = jax.random.randint(key_first, (TOKENS,), 0, per_group)
    second_pick = (first_pick + jax.random.randint(key_second, (TOKENS,), 1, per_group)) % per_group
    return jnp.stack([group_ids * per_group + first_pick, group_ids * per_group + second_pick], axis=1).astype(jnp.int32)


def draw_residual_in(key, part):
    key_base, key_rows = jax.random.split(jax.random.fold_in(key, 23), 2)
    column_scale = jnp.exp(jnp.linspace(math.log(0.3), math.log(3.0), D)).astype(jnp.float32)
    row_scale = jnp.exp(jax.random.uniform(key_rows, (TOKENS, 1), jnp.float32, math.log(0.4), math.log(4.0)))
    base = jnp.clip(jax.random.normal(key_base, (TOKENS, D), jnp.float32), -4.0, 4.0)
    return (base * row_scale * column_scale[None, :]).astype(jnp.bfloat16)


def level_of(key, extent, cuts, low, largest):
    def one(axis_at, shards_of):
        draws = jax.random.uniform(jax.random.fold_in(jax.random.fold_in(key, 6), axis_at), (shards_of,), jnp.float32, low / len(cuts), largest / len(cuts))
        return jnp.repeat(jnp.exp(draws), extent[axis_at] // shards_of).reshape((-1,) + (1,) * (len(extent) - axis_at - 1))

    factor_of = one(*cuts[0])
    for cut in cuts[1:]:
        factor_of = factor_of * one(*cut)
    return factor_of


def profile(amount, total, reach, skew):
    weights = [(1 << 20) // math.isqrt(standing ** skew) + 1 for standing in range(2, amount + 1)]
    spare, counts = total - reach - (amount - 1), [1] * (amount - 1)
    while spare > 0:
        candidates = [i for i in range(amount - 1) if counts[i] < reach]
        mass, budget = sum([weights[i] for i in candidates]), spare
        for i in candidates:
            extra = min(reach - counts[i], max(1, budget * weights[i] // mass), spare)
            counts[i] = counts[i] + extra
            spare = spare - extra
    return np.array([reach] + counts)


def uneven_parts(rng, count, total, most, lean):
    if count == 2:
        one = jax.random.randint(rng, (), max(1, total - most), min(most, total - 1) + 1)
        return jnp.stack([one, total - one])
    sizes = jnp.asarray(profile(count, total, most, lean), jnp.int32)
    couples = (count - 1) // 2
    giver, sink = sizes[1:1 + 2 * couples:2], sizes[2:2 + 2 * couples:2]
    margin = jnp.minimum(giver - 1, most - sink)
    passed = jax.random.randint(jax.random.fold_in(rng, 1), (couples,), 0, 1 << 20) % (margin + 1)
    sizes = sizes.at[1:1 + 2 * couples:2].set(giver - passed).at[2:2 + 2 * couples:2].set(sink + passed)
    return sizes[jax.random.permutation(jax.random.fold_in(rng, 2), count)]


def normal_values(stream_key, dims, scale, most, cuts=(), held_as=jnp.bfloat16):
    loudness = level_of(stream_key, dims, cuts, -0.22, 0.18) if cuts else 1.0
    values = jax.random.normal(stream_key, dims, jnp.float32) * scale * loudness
    return jnp.minimum(jnp.maximum(values, -most), most).astype(held_as)


def setup_inputs(seed: int = 0) -> dict:
    splits = jax.random.split(jax.random.key(seed), 14)
    b_gate = normal_values(splits[0], (TOKENS, CH), 1.0, 6.0, ((0, 32), (1, 16)))
    c_gate = normal_values(splits[1], (TOKENS, CH), 1.0, 6.0, ((0, 32), (1, 16)))
    h_in = normal_values(splits[2], (TOKENS, CH), 1.0, 6.0, ((0, 32), (1, 16)))
    docs = jnp.searchsorted(jnp.cumsum(uneven_parts(splits[3], N_SP // 2, TOKENS, 4 * TOK_DEV, 1)), jnp.arange(TOKENS), side="right").astype(jnp.int32)
    conv_taps = normal_values(splits[4], (3, CH), 0.577, 3.0)
    out_weight = normal_values(splits[5], (CH, D), CH ** -0.5, 0.1875, ((1, 16),))
    residual_in = draw_residual_in(jax.random.fold_in(splits[13], 71), 0)
    norm_gain = jnp.clip(1.0 + 0.18 * jax.random.normal(splits[7], (D,), jnp.float32), 0.099609375, 1.8984375).astype(jnp.bfloat16)
    expert_pick = draw_expert_pick(jax.random.fold_in(splits[13], 71), 0)
    route_weight = jnp.clip(jnp.exp(math.log(2.0) - 1.3862944 * jax.random.uniform(splits[9], (TOKENS, TOP_K), jnp.float32) ** level_of(splits[9], (TOKENS, TOP_K), ((0, 32),), -0.2, 0.2)), 0.5, 2.0)
    w_gate = normal_values(splits[10], (EXPERTS, D, FFE), D ** -0.5, 0.09375, ((0, 32), (2, 16)))
    w_up = normal_values(splits[11], (EXPERTS, D, FFE), D ** -0.5, 0.09375, ((0, 32), (2, 16)))
    w_down = normal_values(splits[12], (EXPERTS, FFE, D), FFE ** -0.5, 0.125, ((0, 32), (2, 16)))
    return {"b_gate": b_gate, "c_gate": c_gate, "h_in": h_in, "docs": docs, "conv_taps": conv_taps, "out_weight": out_weight, "residual_in": residual_in, "norm_gain": norm_gain, "expert_pick": expert_pick, "route_weight": route_weight, "w_gate": w_gate, "w_up": w_up, "w_down": w_down}


NORM_EPS = 1e-06

def reference(b_gate, c_gate, h_in, docs, conv_taps, out_weight, residual_in, norm_gain, expert_pick, route_weight, w_gate, w_up, w_down):
    product = (c_gate.astype(jnp.float32) * h_in.astype(jnp.float32)).astype(jnp.bfloat16)
    product_f = product.astype(jnp.float32)
    tap_weights = conv_taps.astype(jnp.float32)
    conv_sum = tap_weights[0][None, :] * product_f
    for step_back in (1, 2):
        earlier = jnp.concatenate([jnp.zeros((step_back, CH), jnp.float32), product_f[:-step_back]], axis=0)
        earlier_doc = jnp.concatenate([jnp.full((step_back,), -1, jnp.int32), docs[:-step_back]], axis=0)
        same_doc = (earlier_doc == docs).astype(jnp.float32)[:, None]
        conv_sum = conv_sum + tap_weights[step_back][None, :] * earlier * same_doc
    conv_out = (b_gate.astype(jnp.float32) * conv_sum).astype(jnp.bfloat16)
    stream = (residual_in.astype(jnp.float32) + jnp.dot(conv_out, out_weight, preferred_element_type=jnp.float32)).astype(jnp.bfloat16)
    stream_f = stream.astype(jnp.float32)
    inverse = lax.rsqrt(lax.optimization_barrier(jnp.mean(stream_f * stream_f, axis=1, keepdims=True)) + NORM_EPS)
    normed = (stream_f * inverse * norm_gain.astype(jnp.float32)[None, :]).astype(jnp.bfloat16)
    per_block = expert_pick.reshape(N_SP, TOK_DEV * TOP_K)
    onehot = (per_block[:, :, None] == jnp.arange(EXPERTS, dtype=jnp.int32)[None, None, :]).astype(jnp.int32)
    slot_pos = lax.optimization_barrier(jnp.sum((jnp.cumsum(onehot, axis=1) - onehot) * onehot, axis=2))
    kept_mask = slot_pos < CAP
    block_ids = jnp.arange(N_SP, dtype=jnp.int32)[:, None]
    target = (per_block * N_SP + block_ids) * CAP + jnp.minimum(slot_pos, CAP - 1)
    target = jnp.where(kept_mask, target, EXPERTS * N_SP * CAP).astype(jnp.int32)
    assign_ids = jnp.arange(N_SP * TOK_DEV * TOP_K, dtype=jnp.int32).reshape(N_SP, TOK_DEV * TOP_K)
    table = jnp.full((EXPERTS * N_SP * CAP + 1,), -1, jnp.int32).at[target.reshape(-1)].set(assign_ids.reshape(-1))
    table = table[:-1].reshape(EXPERTS, N_SP * CAP)
    weights_flat = route_weight.reshape(-1)

    def one_expert(running, expert):
        sources = table[expert]
        filled = sources >= 0
        safe_ids = jnp.maximum(sources, 0)
        token_ids = safe_ids // TOP_K
        inputs = jnp.where(filled[:, None], normed[token_ids], jnp.zeros((), normed.dtype))
        gate_pre = jnp.dot(inputs, w_gate[expert], preferred_element_type=jnp.float32)
        up_pre = jnp.dot(inputs, w_up[expert], preferred_element_type=jnp.float32)
        hidden = (jax.nn.silu(gate_pre) * up_pre).astype(jnp.bfloat16)
        result = jnp.dot(hidden, w_down[expert], preferred_element_type=jnp.float32).astype(jnp.bfloat16)
        factor = jnp.where(filled, weights_flat[safe_ids], jnp.zeros((), weights_flat.dtype))
        scaled = result.astype(jnp.float32) * factor[:, None]
        return (running.at[token_ids].add(scaled), None)
    feed_out, unused = lax.scan(one_expert, jnp.zeros((TOKENS, D), jnp.float32), jnp.arange(EXPERTS, dtype=jnp.int32))
    return (stream_f + feed_out).astype(jnp.bfloat16)
```

```python
import jax
import jax.numpy as jnp
from jax import lax
from jax.experimental import pallas as pl
from jax.experimental.pallas import tpu as pltpu
from jax.sharding import Mesh
from jax.sharding import PartitionSpec as P

TP = ("ty", "tx")
NORM_EPS = 1e-06
F32 = jnp.float32
BF16 = jnp.bfloat16


def dot(a, b, ca=1, cb=0):
    return lax.dot_general(a, b, (((ca,), (cb,)), ((), ())), preferred_element_type=F32)


def iota(shape, dim):
    return lax.broadcasted_iota(jnp.int32, shape, dim)


def to_row(col, width, offset):
    rows = col.shape[0]
    hit = iota((rows, width), 0) == iota((rows, width), 1) + offset
    return jnp.sum(jnp.where(hit, col, jnp.zeros((), col.dtype)), axis=0, keepdims=True)


def to_col(row, rows, offset):
    width = row.shape[1]
    hit = iota((rows, width), 0) == iota((rows, width), 1) + offset
    return jnp.sum(jnp.where(hit, row, jnp.zeros((), row.dtype)), axis=1, keepdims=True)


def routing(pick, n_exp, cap, n_z):
    toks = pick.shape[0]
    rows = n_exp * cap
    half = rows // 2

    def body(pick_ref, c0_ref, c1_ref, ct_ref, split_ref, join_ref):
        e0 = pick_ref[:, 0:1]
        e1 = pick_ref[:, 1:2]
        experts = iota((toks, 128), 1)
        oh0 = (experts == e0).astype(F32)
        oh1 = (experts == e1).astype(F32)
        earlier = (iota((toks, toks), 0) > iota((toks, toks), 1)).astype(F32).astype(BF16)
        count = dot(earlier, (oh0 + oh1).astype(BF16))
        s0 = jnp.sum(count * oh0, axis=1, keepdims=True).astype(jnp.int32)
        s1 = jnp.sum((count + oh0) * oh1, axis=1, keepdims=True).astype(jnp.int32)
        t0 = jnp.where(s0 < cap, e0 * cap + s0, -1)
        t1 = jnp.where(s1 < cap, e1 * cap + s1, -1)
        lanes = iota((toks, rows), 1)
        c0_ref[...] = (lanes == t0).astype(F32).astype(BF16)
        c1_ref[...] = (lanes == t1).astype(F32).astype(BF16)
        r0 = to_row(t0, toks, 0)
        r1 = to_row(t1, toks, 0)
        down = iota((rows, toks), 0)
        ct_ref[...] = jnp.logical_or(down == r0, down == r1).astype(F32).astype(BF16)
        q = iota((rows, 1), 0)
        core = (q >= half).astype(jnp.int32)
        within = q - core * half
        z = (within * (65536 // cap + 1)) >> 16
        src = within + z * cap + core * cap
        split_ref[...] = (iota((rows, rows), 1) == src).astype(F32).astype(BF16)
        z2 = (q * (65536 // (2 * cap) + 1)) >> 16
        rest = q - z2 * (2 * cap)
        core2 = (rest >= cap).astype(jnp.int32)
        src2 = core2 * half + z2 * cap + rest - core2 * cap
        join_ref[...] = (iota((rows, rows), 1) == src2).astype(F32).astype(BF16)

    return pl.pallas_call(
        body,
        out_shape=(
            jax.ShapeDtypeStruct((toks, rows), BF16),
            jax.ShapeDtypeStruct((toks, rows), BF16),
            jax.ShapeDtypeStruct((rows, toks), BF16),
            jax.ShapeDtypeStruct((rows, rows), BF16),
            jax.ShapeDtypeStruct((rows, rows), BF16),
        ),
        name="routing",
    )(pick)


def project(conv_all, out_weight, residual, ct):
    toks, width = residual.shape
    rows = ct.shape[0]

    def body(conv_ref, w_ref, res_ref, ct_ref, stream_ref, out_ref):
        stream = (res_ref[...].astype(F32) + dot(conv_ref[...], w_ref[...], 0, 0)).astype(BF16)
        stream_ref[...] = stream
        out_ref[...] = dot(ct_ref[...], stream).astype(BF16)

    return pl.pallas_call(
        body,
        out_shape=(
            jax.ShapeDtypeStruct((toks, width), BF16),
            jax.ShapeDtypeStruct((rows, width), BF16),
        ),
        name="project",
    )(conv_all, out_weight, residual, ct)


def split_rows(got, split, n_tx):
    rows, width = got.shape
    half = rows // 2

    def body(got_ref, split_ref, out_ref):
        both = dot(split_ref[...], got_ref[...]).astype(BF16)
        for core in range(2):
            for t in range(n_tx):
                out_ref[core * n_tx + t] = both[core * half : (core + 1) * half]

    return pl.pallas_call(
        body, out_shape=jax.ShapeDtypeStruct((2 * n_tx, half, width), BF16), name="split_rows"
    )(got, split)


def gate_up(where, x, gain, w_gate, w_up, pieces):
    n_ty = len(pieces) + 1
    groups, half, width = x.shape
    n_tx = groups // 2
    feats = n_tx * width
    hid = w_gate.shape[1]
    rows = 2 * half

    def body(at_ref, x_ref, gain_ref, wg_ref, wu_ref, *rest):
        piece_refs, out_ref = rest[:-1], rest[-1]
        ty = at_ref[0]
        gain_row = gain_ref[...].astype(F32)
        extra = jnp.zeros((8, 2 * hid), F32)
        place = iota((8, 2 * hid), 0)
        for core in range(2):
            raw = jnp.concatenate([x_ref[core * n_tx + t] for t in range(n_tx)], axis=1).astype(F32)
            squares = jnp.sum(raw * raw, axis=1, keepdims=True)
            y = (raw * gain_row).astype(BF16)
            for k in range(2):
                row = to_row(squares, 2 * hid, k * 2 * hid)
                high = row.astype(BF16).astype(F32)
                at = core * 2 + k
                extra = jnp.where(place == at, high, extra)
                extra = jnp.where(place == at + 4, row - high, extra)
            keep = pl.ds(core * half, half)
            out_ref[ty, keep, 0:hid] = dot(y, wg_ref[...]).astype(BF16)
            out_ref[ty, keep, hid : 2 * hid] = dot(y, wu_ref[...]).astype(BF16)
            for d in range(1, n_ty):
                to = lax.rem(ty + (n_ty - d), n_ty)
                out_ref[to, keep, :] = dot(y, piece_refs[d - 1][...]).astype(BF16)
        for to in range(n_ty):
            out_ref[to, rows : rows + 8, :] = extra.astype(BF16)

    full = lambda shape: pl.BlockSpec(shape, lambda i, at: (0,) * len(shape))
    return pl.pallas_call(
        body,
        grid_spec=pltpu.PrefetchScalarGridSpec(
            num_scalar_prefetch=1,
            grid=(1,),
            in_specs=[
                full(x.shape),
                pl.BlockSpec((1, feats), lambda i, at: (0, at[0])),
                pl.BlockSpec((feats, hid), lambda i, at: (at[0], 0)),
                pl.BlockSpec((feats, hid), lambda i, at: (at[0], 0)),
                *[full(p.shape) for p in pieces],
            ],
            out_specs=full((n_ty, rows + 8, 2 * hid)),
        ),
        out_shape=jax.ShapeDtypeStruct((n_ty, rows + 8, 2 * hid), BF16),
        name="gate_up",
    )(where, x, gain, w_gate, w_up, *pieces)


def activate(parts, full_dim):
    n_ty, padded, both = parts.shape
    rows, hid = padded - 8, both // 2
    half = rows // 2

    def body(p_ref, out_ref):
        extra = sum(p_ref[k, rows : rows + 8, :].astype(F32) for k in range(n_ty))
        for core in range(2):
            keep = pl.ds(core * half, half)
            total = sum(p_ref[k, keep, :].astype(F32) for k in range(n_ty))
            squares = jnp.zeros((half, 1), F32)
            for k in range(2):
                at = core * 2 + k
                row = extra[at : at + 1] + extra[at + 4 : at + 5]
                squares = squares + to_col(row, half, k * both)
            total = total * lax.rsqrt(squares / full_dim + NORM_EPS)
            gate, up = total[:, :hid], total[:, hid:]
            hidden = (gate / (1.0 + jnp.exp(-gate)) * up).astype(BF16)
            for k in range(n_ty):
                out_ref[k, keep, :] = hidden

    return pl.pallas_call(
        body, out_shape=jax.ShapeDtypeStruct((n_ty, rows, hid), BF16), name="activate"
    )(parts)


def down(where, hidden, w_down, pieces):
    n_ty, rows, hid = hidden.shape
    n_tx = len(pieces) + 1
    half = rows // 2
    width = w_down.shape[-1]

    def body(at_ref, h_ref, wd_ref, *rest):
        piece_refs, out_ref = rest[:-1], rest[-1]
        tx = at_ref[1]
        h = jnp.concatenate([h_ref[k] for k in range(n_ty)], axis=1)
        for d in range(n_tx):
            w = (wd_ref[...] if d == 0 else piece_refs[d - 1][...]).reshape(n_ty * hid, width)
            part = dot(h, w).astype(BF16)
            to = lax.rem(tx + (n_tx - d), n_tx)
            out_ref[to] = part[:half]
            out_ref[n_tx + to] = part[half:]

    full = lambda shape: pl.BlockSpec(shape, lambda i, at: (0,) * len(shape))
    return pl.pallas_call(
        body,
        grid_spec=pltpu.PrefetchScalarGridSpec(
            num_scalar_prefetch=1,
            grid=(1,),
            in_specs=[
                full(hidden.shape),
                pl.BlockSpec((n_ty, 1, hid, width), lambda i, at: (0, at[1], 0, 0)),
                *[full(p.shape) for p in pieces],
            ],
            out_specs=full((2 * n_tx, half, width)),
        ),
        out_shape=jax.ShapeDtypeStruct((2 * n_tx, half, width), BF16),
        name="down",
    )(where, hidden, w_down, *pieces)


def join_rows(parts, join):
    groups, half, width = parts.shape
    n_tx = groups // 2

    def body(p_ref, join_ref, out_ref):
        whole = [
            sum(p_ref[core * n_tx + t].astype(F32) for t in range(n_tx)).astype(BF16)
            for core in range(2)
        ]
        out_ref[...] = dot(join_ref[...], jnp.concatenate(whole, axis=0)).astype(BF16)

    return pl.pallas_call(
        body, out_shape=jax.ShapeDtypeStruct((2 * half, width), BF16), name="join_rows"
    )(parts, join)


def combine(back, c0, c1, weights, stream):
    def body(back_ref, c0_ref, c1_ref, w_ref, stream_ref, out_ref):
        rows = back_ref[...]
        feed = dot(c0_ref[...], rows) * w_ref[:, 0:1] + dot(c1_ref[...], rows) * w_ref[:, 1:2]
        out_ref[...] = (stream_ref[...].astype(F32) + feed).astype(BF16)

    return pl.pallas_call(
        body, out_shape=jax.ShapeDtypeStruct(stream.shape, BF16), name="combine"
    )(back, c0, c1, weights, stream)


def local(
    b_gate,
    c_gate,
    h_in,
    docs,
    conv_taps,
    out_weight,
    residual_in,
    norm_gain,
    expert_pick,
    route_weight,
    w_gate,
    w_up,
    w_down,
):
    toks, chans = h_in.shape
    width = residual_in.shape[1]
    full_dim = w_gate.shape[1]
    hid = w_gate.shape[2]
    n_z, n_ty, n_tx = (lax.axis_size(a) for a in ("z", "ty", "tx"))
    n_sp = 2 * n_z
    cap = 5 * toks // (2 * n_sp)
    rows = n_sp * cap
    half = rows // 2
    sp_index = lax.axis_index(("z", "core"))
    ty, tx = lax.axis_index("ty"), lax.axis_index("tx")
    tp_index = ty * n_tx + tx
    where = jnp.stack([ty, tx]).astype(jnp.int32)

    product = (c_gate.astype(F32) * h_in.astype(F32)).astype(BF16)
    edge = lax.ppermute(
        product[toks - 2 :], ("z", "core"), [(i, i + 1) for i in range(n_sp - 1)]
    )
    first_pos = sp_index * toks
    padded_docs = jnp.concatenate([jnp.full((2,), -1, jnp.int32), docs], axis=0)
    near = lax.dynamic_slice_in_dim(padded_docs, first_pos, toks + 2)
    taps = lax.dynamic_slice_in_dim(conv_taps, tp_index * chans, chans, 1).astype(F32)
    extended = jnp.concatenate([edge, product], axis=0).astype(F32)
    conv_sum = taps[0][None, :] * extended[2:]
    for back in (1, 2):
        same = (near[2 - back : 2 - back + toks] == near[2:]).astype(F32)[:, None]
        conv_sum = conv_sum + taps[back][None, :] * extended[2 - back : 2 - back + toks] * same
    conv = (b_gate.astype(F32) * conv_sum).astype(BF16)
    n_tp = n_ty * n_tx
    conv_all = lax.all_to_all(
        jnp.broadcast_to(conv.T[None], (n_tp, chans, toks)), TP, 0, 0, tiled=True
    ).reshape(n_tp * chans, toks)

    feats = full_dim // n_ty
    w_both = [w.reshape(n_ty, feats, hid) for w in (w_gate[0], w_up[0])]
    gate_up_pieces = []
    for d in range(1, n_ty):
        to = lax.rem(ty + d, n_ty)
        piece = jnp.concatenate(
            [lax.dynamic_index_in_dim(w, to, 0, keepdims=False) for w in w_both], axis=1
        )
        gate_up_pieces.append(
            lax.ppermute(piece, "ty", [(i, (i + d) % n_ty) for i in range(n_ty)])
        )
    w_down4 = w_down[0].reshape(n_ty, n_tx, hid, width)
    down_pieces = []
    for d in range(1, n_tx):
        to = lax.rem(tx + d, n_tx)
        piece = lax.dynamic_index_in_dim(w_down4, to, 1, keepdims=False)
        down_pieces.append(lax.ppermute(piece, "tx", [(i, (i + d) % n_tx) for i in range(n_tx)]))

    c0, c1, ct, split, join = routing(expert_pick, n_sp, cap, n_z)
    stream, outgoing = project(conv_all, out_weight, residual_in, ct)
    got = lax.all_to_all(
        outgoing.reshape(n_z, 2 * cap, width), "z", 0, 0, tiled=True
    ).reshape(rows, width)
    x = lax.all_to_all(split_rows(got, split, n_tx), ("core", "tx"), 0, 0, tiled=True)
    parts = gate_up(where, x, norm_gain.reshape(1, -1), w_gate[0], w_up[0], gate_up_pieces)
    parts = lax.all_to_all(parts, "ty", 0, 0, tiled=True)
    hidden = lax.all_to_all(activate(parts, full_dim), "ty", 0, 0, tiled=True)
    outs = lax.all_to_all(
        down(where, hidden, w_down4, down_pieces), ("core", "tx"), 0, 0, tiled=True
    )
    back = lax.all_to_all(
        join_rows(outs, join).reshape(n_z, 2 * cap, width), "z", 0, 0, tiled=True
    ).reshape(rows, width)
    return combine(back, c0, c1, route_weight, stream)


def solution(mesh):
    finer = Mesh(
        mesh.devices.reshape(mesh.shape["sp"] // 2, 2, 4, 4), ("z", "core", "ty", "tx")
    )
    sp = ("z", "core")
    placed = (
        P(sp, TP),
        P(sp, TP),
        P(sp, TP),
        P(),
        P(),
        P(None, TP),
        P(sp, TP),
        P(),
        P(sp, None),
        P(sp, None),
        P(sp, None, TP),
        P(sp, None, TP),
        P(sp, None, TP),
    )
    return jax.shard_map(local, mesh=finer, in_specs=placed, out_specs=P(sp, TP), check_vma=False)
```

```python
import jax
import jax.numpy as jnp
from jax import lax
from jax.experimental import pallas as pl
from jax.experimental.pallas import tpu as pltpu
from jax.sharding import Mesh
from jax.sharding import PartitionSpec as P

TP = ("ty", "tx")
NORM_EPS = 1e-06
F32 = jnp.float32
BF16 = jnp.bfloat16


def dot(a, b, ca=1, cb=0):
    return lax.dot_general(a, b, (((ca,), (cb,)), ((), ())), preferred_element_type=F32)


def kernel(body, outs, name, *args, limit=12):
    held = [a if a.ndim == 1 else pltpu.with_memory_space_constraint(a, pltpu.VMEM) for a in args]
    vmem = pl.BlockSpec(memory_space=pltpu.VMEM)
    smem = pl.BlockSpec(memory_space=pltpu.SMEM)
    got = pl.pallas_call(
        body,
        out_shape=tuple(jax.ShapeDtypeStruct(o, BF16) for o in outs),
        in_specs=[smem if a.ndim == 1 else vmem for a in args],
        out_specs=tuple(vmem for o in outs),
        compiler_params=pltpu.CompilerParams(vmem_limit_bytes=limit << 20),
        name=name,
    )(*held)
    return got if len(outs) > 1 else got[0]


def iota(shape, dim):
    return lax.broadcasted_iota(jnp.int32, shape, dim)


def to_row(col, width, offset):
    rows = col.shape[0]
    hit = iota((rows, width), 0) == iota((rows, width), 1) + offset
    return jnp.sum(jnp.where(hit, col, jnp.zeros((), col.dtype)), axis=0, keepdims=True)


def to_col(row, rows, offset):
    width = row.shape[1]
    hit = iota((rows, width), 0) == iota((rows, width), 1) + offset
    return jnp.sum(jnp.where(hit, row, jnp.zeros((), row.dtype)), axis=1, keepdims=True)


def slots(pick_ref, cap):
    toks = pick_ref.shape[0]
    e0 = pick_ref[:, 0:1]
    e1 = pick_ref[:, 1:2]
    experts = iota((toks, 128), 1)
    oh0 = (experts == e0).astype(F32)
    oh1 = (experts == e1).astype(F32)
    earlier = (iota((toks, toks), 0) > iota((toks, toks), 1)).astype(F32).astype(BF16)
    count = dot(earlier, (oh0 + oh1).astype(BF16))
    s0 = jnp.sum(count * oh0, axis=1, keepdims=True).astype(jnp.int32)
    s1 = jnp.sum((count + oh0) * oh1, axis=1, keepdims=True).astype(jnp.int32)
    return jnp.where(s0 < cap, e0 * cap + s0, -1), jnp.where(s1 < cap, e1 * cap + s1, -1)


def routing_out(pick, rows, cap):
    toks = pick.shape[0]

    def body(pick_ref, ct_ref):
        t0, t1 = slots(pick_ref, cap)
        r0 = to_row(t0, toks, 0)
        r1 = to_row(t1, toks, 0)
        across = iota((rows, toks), 0)
        ct_ref[...] = jnp.logical_or(across == r0, across == r1).astype(F32).astype(BF16)

    return kernel(body, ((rows, toks),), "routing_out", pick)


def routing_back(pick, rows, cap):
    toks = pick.shape[0]

    def body(pick_ref, c0_ref, c1_ref):
        t0, t1 = slots(pick_ref, cap)
        lanes = iota((toks, rows), 1)
        c0_ref[...] = (lanes == t0).astype(F32).astype(BF16)
        c1_ref[...] = (lanes == t1).astype(F32).astype(BF16)

    return kernel(body, ((toks, rows), (toks, rows)), "routing_back", pick)


def project(conv_all, out_weight, residual, ct):
    toks, width = residual.shape
    rows = ct.shape[0]

    def body(conv_ref, w_ref, res_ref, ct_ref, stream_ref, out_ref):
        stream = (res_ref[...].astype(F32) + dot(conv_ref[...], w_ref[...], 0, 0)).astype(BF16)
        stream_ref[...] = stream
        out_ref[...] = dot(ct_ref[...], stream).astype(BF16)

    outs = ((toks, width), (rows, width))
    return kernel(body, outs, "project", conv_all, out_weight, residual, ct)


def order_map(cap, block, splitting):
    q = iota((block, 1), 0)
    if splitting:
        core = (q >= block // 2).astype(jnp.int32)
        within = q - core * (block // 2)
        z = (within * (65536 // cap + 1)) >> 16
        source = within + z * cap + core * cap
    else:
        z = (q * (65536 // (2 * cap) + 1)) >> 16
        rest = q - z * (2 * cap)
        core = (rest >= cap).astype(jnp.int32)
        source = core * (block // 2) + z * cap + rest - core * cap
    return (iota((block, block), 1) == source).astype(F32).astype(BF16)


def split_rows(got, n_tx, cap):
    rows, width = got.shape
    half = rows // 2
    block = 8 * cap
    part = block // 2

    def body(got_ref, out_ref):
        order = order_map(cap, block, True)
        for i in range(rows // block):
            both = dot(order, got_ref[i * block : (i + 1) * block]).astype(BF16)
            for core in range(2):
                for t in range(n_tx):
                    out_ref[core * n_tx + t, i * part : (i + 1) * part] = both[
                        core * part : (core + 1) * part
                    ]

    return kernel(body, ((2 * n_tx, half, width),), "split_rows", got)


def gate_up(where, x, gain, w_gate, w_up, pieces):
    n_ty = len(pieces) + 1
    groups, half, width = x.shape
    n_tx = groups // 2
    feats = n_tx * width
    hid = w_gate.shape[1]
    rows = 2 * half

    def body(at_ref, x_ref, gain_ref, wg_ref, wu_ref, *rest):
        piece_refs, out_refs = rest[: n_ty - 1], rest[n_ty - 1 :]
        mine = pl.ds(pl.multiple_of(at_ref[0] * feats, feats), feats)
        gain_row = gain_ref[:, mine].astype(F32)
        extra = jnp.zeros((8, 2 * hid), F32)
        place = iota((8, 2 * hid), 0)
        for core in range(2):
            raw = jnp.concatenate([x_ref[core * n_tx + t] for t in range(n_tx)], axis=1).astype(F32)
            squares = jnp.sum(raw * raw, axis=1, keepdims=True)
            y = (raw * gain_row).astype(BF16)
            for k in range(2):
                row = to_row(squares, 2 * hid, k * 2 * hid)
                high = row.astype(BF16).astype(F32)
                at = core * 2 + k
                extra = jnp.where(place == at, high, extra)
                extra = jnp.where(place == at + 4, row - high, extra)
            keep = slice(core * half, (core + 1) * half)
            out_refs[0][keep, 0:hid] = dot(y, wg_ref[mine, :]).astype(BF16)
            out_refs[0][keep, hid : 2 * hid] = dot(y, wu_ref[mine, :]).astype(BF16)
            for d in range(1, n_ty):
                out_refs[d][keep, :] = dot(y, piece_refs[d - 1][...]).astype(BF16)
        for out_ref in out_refs:
            out_ref[rows : rows + 8, :] = extra.astype(BF16)

    outs = tuple((rows + 8, 2 * hid) for d in range(n_ty))
    return kernel(body, outs, "gate_up", where, x, gain, w_gate, w_up, *pieces, limit=24)


def activate(parts, full_dim):
    padded, both = parts[0].shape
    rows, hid = padded - 8, both // 2
    half = rows // 2

    def body(*refs):
        p_refs, out_ref = refs[:-1], refs[-1]
        extra = sum(p[rows : rows + 8, :].astype(F32) for p in p_refs)
        for core in range(2):
            keep = slice(core * half, (core + 1) * half)
            total = sum(p[keep, :].astype(F32) for p in p_refs)
            squares = jnp.zeros((half, 1), F32)
            for k in range(2):
                at = core * 2 + k
                row = extra[at : at + 1] + extra[at + 4 : at + 5]
                squares = squares + to_col(row, half, k * both)
            total = total * lax.rsqrt(squares / full_dim + NORM_EPS)
            gate, up = total[:, :hid], total[:, hid:]
            out_ref[keep, :] = (gate / (1.0 + jnp.exp(-gate)) * up).astype(BF16)

    return kernel(body, ((rows, hid),), "activate", *parts)


def down(where, hidden, w_down, pieces):
    n_ty = len(hidden)
    rows, hid = hidden[0].shape
    n_tx = len(pieces) + 1
    half = rows // 2
    width = w_down.shape[-1]

    def body(at_ref, wd_ref, *rest):
        h_refs, piece_refs, out_ref = rest[:n_ty], rest[n_ty:-1], rest[-1]
        ty, tx = at_ref[0], at_ref[1]
        h = jnp.concatenate([r[...] for r in h_refs], axis=1)
        blocks = [lax.rem(ty + (n_ty - d), n_ty) for d in range(n_ty)]
        for d in range(n_tx):
            if d == 0:
                w = [wd_ref[b, tx] for b in blocks]
            else:
                w = [piece_refs[d - 1][b] for b in blocks]
            part = dot(h, jnp.concatenate(w, axis=0)).astype(BF16)
            to = lax.rem(tx + (n_tx - d), n_tx)
            out_ref[to] = part[:half]
            out_ref[n_tx + to] = part[half:]

    outs = ((2 * n_tx, half, width),)
    return kernel(body, outs, "down", where, w_down, *hidden, *pieces, limit=24)


def join_rows(parts, cap):
    groups, half, width = parts.shape
    n_tx = groups // 2
    block = 8 * cap
    part = block // 2

    def body(p_ref, out_ref):
        order = order_map(cap, block, False)
        for i in range(2 * half // block):
            keep = slice(i * part, (i + 1) * part)
            both = [
                sum(p_ref[core * n_tx + t, keep].astype(F32) for t in range(n_tx)).astype(BF16)
                for core in range(2)
            ]
            out_ref[i * block : (i + 1) * block] = dot(
                order, jnp.concatenate(both, axis=0)
            ).astype(BF16)

    return kernel(body, ((2 * half, width),), "join_rows", parts)


def combine(back, c0, c1, weights, stream):
    def body(back_ref, c0_ref, c1_ref, w_ref, stream_ref, out_ref):
        rows = back_ref[...]
        feed = dot(c0_ref[...], rows) * w_ref[:, 0:1] + dot(c1_ref[...], rows) * w_ref[:, 1:2]
        out_ref[...] = (stream_ref[...].astype(F32) + feed).astype(BF16)

    return kernel(body, (stream.shape,), "combine", back, c0, c1, weights, stream)


def shifted(value, axis, steps):
    count = lax.axis_size(axis)
    return lax.ppermute(value, axis, [(i, (i + steps) % count) for i in range(count)])


def local(
    b_gate,
    c_gate,
    h_in,
    docs,
    conv_taps,
    out_weight,
    residual_in,
    norm_gain,
    expert_pick,
    route_weight,
    w_gate,
    w_up,
    w_down,
):
    toks, chans = h_in.shape
    width = residual_in.shape[1]
    full_dim = w_gate.shape[1]
    hid = w_gate.shape[2]
    n_z, n_ty, n_tx = (lax.axis_size(a) for a in ("z", "ty", "tx"))
    n_sp = 2 * n_z
    cap = 5 * toks // (2 * n_sp)
    rows = n_sp * cap
    sp_index = lax.axis_index(("z", "core"))
    ty, tx = lax.axis_index("ty"), lax.axis_index("tx")
    tp_index = ty * n_tx + tx
    where = jnp.stack([ty, tx]).astype(jnp.int32)

    product = (c_gate.astype(F32) * h_in.astype(F32)).astype(BF16)
    edge = lax.ppermute(
        product[toks - 2 :], ("z", "core"), [(i, i + 1) for i in range(n_sp - 1)]
    )
    first_pos = sp_index * toks
    padded_docs = jnp.concatenate([jnp.full((2,), -1, jnp.int32), docs], axis=0)
    near = lax.dynamic_slice_in_dim(padded_docs, first_pos, toks + 2)
    taps = lax.dynamic_slice_in_dim(conv_taps, tp_index * chans, chans, 1).astype(F32)
    extended = jnp.concatenate([edge, product], axis=0).astype(F32)
    conv_sum = taps[0][None, :] * extended[2:]
    for back in (1, 2):
        same = (near[2 - back : 2 - back + toks] == near[2:]).astype(F32)[:, None]
        conv_sum = conv_sum + taps[back][None, :] * extended[2 - back : 2 - back + toks] * same
    conv = (b_gate.astype(F32) * conv_sum).astype(BF16)
    n_tp = n_ty * n_tx
    conv_all = lax.all_to_all(
        jnp.broadcast_to(conv.T[None], (n_tp, chans, toks)), TP, 0, 0, tiled=True
    ).reshape(n_tp * chans, toks)

    feats = full_dim // n_ty
    w_both = [w.reshape(n_ty, feats, hid) for w in (w_gate[0], w_up[0])]
    gate_up_pieces = []
    for d in range(1, n_ty):
        to = lax.rem(ty + d, n_ty)
        piece = jnp.concatenate(
            [lax.dynamic_index_in_dim(w, to, 0, keepdims=False) for w in w_both], axis=1
        )
        gate_up_pieces.append(shifted(piece, "ty", d))
    w_down4 = w_down[0].reshape(n_ty, n_tx, hid, width)
    down_pieces = []
    for d in range(1, n_tx):
        to = lax.rem(tx + d, n_tx)
        piece = lax.dynamic_index_in_dim(w_down4, to, 1, keepdims=False)
        down_pieces.append(shifted(piece, "tx", d))

    ct = routing_out(expert_pick, rows, cap)
    stream, outgoing = project(conv_all, out_weight, residual_in, ct)
    got = lax.all_to_all(
        outgoing.reshape(n_z, 2 * cap, width), "z", 0, 0, tiled=True
    ).reshape(rows, width)
    got, gate_up_pieces, down_pieces = lax.optimization_barrier(
        (got, gate_up_pieces, down_pieces)
    )
    x = lax.all_to_all(split_rows(got, n_tx, cap), ("core", "tx"), 0, 0, tiled=True)
    parts = gate_up(
        where, x, norm_gain.reshape(1, -1), w_gate[0], w_up[0], gate_up_pieces
    )
    parts = [parts[0]] + [shifted(parts[d], "ty", -d) for d in range(1, n_ty)]
    hidden = activate(parts, full_dim)
    hidden = [hidden] + [shifted(hidden, "ty", d) for d in range(1, n_ty)]
    outs = lax.all_to_all(
        down(where, hidden, w_down4, down_pieces), ("core", "tx"), 0, 0, tiled=True
    )
    outs, late_pick, late_weight = lax.optimization_barrier((outs, expert_pick, route_weight))
    c0, c1 = routing_back(late_pick, rows, cap)
    back = lax.all_to_all(
        join_rows(outs, cap).reshape(n_z, 2 * cap, width), "z", 0, 0, tiled=True
    ).reshape(rows, width)
    return combine(back, c0, c1, late_weight, stream)


def solution(mesh):
    finer = Mesh(
        mesh.devices.reshape(mesh.shape["sp"] // 2, 2, 4, 4), ("z", "core", "ty", "tx")
    )
    sp = ("z", "core")
    placed = (
        P(sp, TP),
        P(sp, TP),
        P(sp, TP),
        P(),
        P(),
        P(None, TP),
        P(sp, TP),
        P(),
        P(sp, None),
        P(sp, None),
        P(sp, None, TP),
        P(sp, None, TP),
        P(sp, None, TP),
    )
    return jax.shard_map(local, mesh=finer, in_specs=placed, out_specs=P(sp, TP), check_vma=False)
```

```python
import jax
import jax.numpy as jnp
from jax import lax
from jax.experimental import pallas as pl
from jax.experimental.pallas import tpu as pltpu
from jax.sharding import Mesh
from jax.sharding import PartitionSpec as P

TP = ("ty", "tx")
NORM_EPS = 1e-06
F32 = jnp.float32
BF16 = jnp.bfloat16


def dot(a, b, ca=1, cb=0):
    return lax.dot_general(a, b, (((ca,), (cb,)), ((), ())), preferred_element_type=F32)


def kernel(body, outs, *args, limit=12):
    held = [a if a.ndim == 1 else pltpu.with_memory_space_constraint(a, pltpu.VMEM) for a in args]
    vmem = pl.BlockSpec(memory_space=pltpu.VMEM)
    smem = pl.BlockSpec(memory_space=pltpu.SMEM)
    got = pl.pallas_call(
        body,
        out_shape=tuple(jax.ShapeDtypeStruct(o, BF16) for o in outs),
        in_specs=[smem if a.ndim == 1 else vmem for a in args],
        out_specs=tuple(vmem for o in outs),
        compiler_params=pltpu.CompilerParams(vmem_limit_bytes=limit << 20),
    )(*held)
    return got if len(outs) > 1 else got[0]


def iota(shape, dim):
    return lax.broadcasted_iota(jnp.int32, shape, dim)


def to_row(col, width, offset):
    rows = col.shape[0]
    hit = iota((rows, width), 0) == iota((rows, width), 1) + offset
    return jnp.sum(jnp.where(hit, col, jnp.zeros((), col.dtype)), axis=0, keepdims=True)


def to_col(row, rows, offset):
    width = row.shape[1]
    hit = iota((rows, width), 0) == iota((rows, width), 1) + offset
    return jnp.sum(jnp.where(hit, row, jnp.zeros((), row.dtype)), axis=1, keepdims=True)


def slots(pick_ref, cap):
    toks = pick_ref.shape[0]
    e0 = pick_ref[:, 0:1]
    e1 = pick_ref[:, 1:2]
    experts = iota((toks, 128), 1)
    oh0 = (experts == e0).astype(F32)
    oh1 = (experts == e1).astype(F32)
    earlier = (iota((toks, toks), 0) > iota((toks, toks), 1)).astype(F32).astype(BF16)
    count = dot(earlier, (oh0 + oh1).astype(BF16))
    s0 = jnp.sum(count * oh0, axis=1, keepdims=True).astype(jnp.int32)
    s1 = jnp.sum((count + oh0) * oh1, axis=1, keepdims=True).astype(jnp.int32)
    return jnp.where(s0 < cap, e0 * cap + s0, -1), jnp.where(s1 < cap, e1 * cap + s1, -1)


def routing_out(pick, rows, cap):
    toks = pick.shape[0]

    def body(pick_ref, ct_ref):
        t0, t1 = slots(pick_ref, cap)
        r0 = to_row(t0, toks, 0)
        r1 = to_row(t1, toks, 0)
        across = iota((rows, toks), 0)
        ct_ref[...] = jnp.logical_or(across == r0, across == r1).astype(F32).astype(BF16)

    return kernel(body, ((rows, toks),), pick)


def routing_back(pick, rows, cap):
    toks = pick.shape[0]

    def body(pick_ref, c0_ref, c1_ref):
        t0, t1 = slots(pick_ref, cap)
        lanes = iota((toks, rows), 1)
        c0_ref[...] = (lanes == t0).astype(F32).astype(BF16)
        c1_ref[...] = (lanes == t1).astype(F32).astype(BF16)

    return kernel(body, ((toks, rows), (toks, rows)), pick)


def project(conv_all, out_weight, residual, ct):
    toks, width = residual.shape
    rows = ct.shape[0]

    def body(conv_ref, w_ref, res_ref, ct_ref, stream_ref, out_ref):
        stream = (res_ref[...].astype(F32) + dot(conv_ref[...], w_ref[...], 0, 0)).astype(BF16)
        stream_ref[...] = stream
        out_ref[...] = dot(ct_ref[...], stream).astype(BF16)

    outs = ((toks, width), (rows, width))
    return kernel(body, outs, conv_all, out_weight, residual, ct)


def order_map(cap, block, splitting):
    q = iota((block, 1), 0)
    if splitting:
        core = (q >= block // 2).astype(jnp.int32)
        within = q - core * (block // 2)
        z = (within * (65536 // cap + 1)) >> 16
        source = within + z * cap + core * cap
    else:
        z = (q * (65536 // (2 * cap) + 1)) >> 16
        rest = q - z * (2 * cap)
        core = (rest >= cap).astype(jnp.int32)
        source = core * (block // 2) + z * cap + rest - core * cap
    return (iota((block, block), 1) == source).astype(F32).astype(BF16)


def split_rows(got, n_tx, cap):
    rows, width = got.shape
    half = rows // 2
    block = 8 * cap
    part = block // 2

    def body(got_ref, out_ref):
        order = order_map(cap, block, True)
        for i in range(rows // block):
            both = dot(order, got_ref[i * block : (i + 1) * block]).astype(BF16)
            for core in range(2):
                for t in range(n_tx):
                    out_ref[core * n_tx + t, i * part : (i + 1) * part] = both[
                        core * part : (core + 1) * part
                    ]

    return kernel(body, ((2 * n_tx, half, width),), got)


def pack(where, w_gate, w_up, n_ty):
    dim, hid = w_gate.shape
    feats = dim // n_ty

    def body(at_ref, wg_ref, wu_ref, *out_refs):
        for d, out_ref in enumerate(out_refs):
            to = lax.rem(at_ref[0] + (d + 1), n_ty)
            rows = pl.ds(pl.multiple_of(to * feats, feats), feats)
            out_ref[:, :hid] = wg_ref[rows, :]
            out_ref[:, hid:] = wu_ref[rows, :]

    outs = tuple((feats, 2 * hid) for _ in range(n_ty - 1))
    return kernel(body, outs, where, w_gate, w_up)


def gate_up(where, x, gain, w_gate, w_up, pieces):
    n_ty = len(pieces) + 1
    groups, half, width = x.shape
    n_tx = groups // 2
    feats = n_tx * width
    hid = w_gate.shape[1]
    rows = 2 * half

    def body(at_ref, x_ref, gain_ref, wg_ref, wu_ref, *rest):
        piece_refs, out_ref = rest[:-1], rest[-1]
        ty = at_ref[0]
        mine = pl.ds(pl.multiple_of(at_ref[0] * feats, feats), feats)
        gain_row = gain_ref[:, mine].astype(F32)
        extra = jnp.zeros((8, 2 * hid), F32)
        place = iota((8, 2 * hid), 0)
        for core in range(2):
            raw = jnp.concatenate([x_ref[core * n_tx + t] for t in range(n_tx)], axis=1).astype(F32)
            squares = jnp.sum(raw * raw, axis=1, keepdims=True)
            y = (raw * gain_row).astype(BF16)
            for k in range(2):
                row = to_row(squares, 2 * hid, k * 2 * hid)
                high = row.astype(BF16).astype(F32)
                at = core * 2 + k
                extra = jnp.where(place == at, high, extra)
                extra = jnp.where(place == at + 4, row - high, extra)
            keep = slice(core * half, (core + 1) * half)
            out_ref[ty, keep, 0:hid] = dot(y, wg_ref[mine, :]).astype(BF16)
            out_ref[ty, keep, hid : 2 * hid] = dot(y, wu_ref[mine, :]).astype(BF16)
            for d in range(1, n_ty):
                to = lax.rem(ty + (n_ty - d), n_ty)
                out_ref[to, keep, :] = dot(y, piece_refs[d - 1][...]).astype(BF16)
        for to in range(n_ty):
            out_ref[to, rows : rows + 8, :] = extra.astype(BF16)

    outs = ((n_ty, rows + 8, 2 * hid),)
    return kernel(body, outs, where, x, gain, w_gate, w_up, *pieces, limit=24)


def activate(parts, full_dim):
    n_ty, padded, both = parts.shape
    rows, hid = padded - 8, both // 2
    half = rows // 2

    def body(p_ref, out_ref):
        extra = sum(p_ref[k, rows : rows + 8, :].astype(F32) for k in range(n_ty))
        for core in range(2):
            keep = slice(core * half, (core + 1) * half)
            total = sum(p_ref[k, keep, :].astype(F32) for k in range(n_ty))
            squares = jnp.zeros((half, 1), F32)
            for k in range(2):
                at = core * 2 + k
                row = extra[at : at + 1] + extra[at + 4 : at + 5]
                squares = squares + to_col(row, half, k * both)
            total = total * lax.rsqrt(squares / full_dim + NORM_EPS)
            gate, up = total[:, :hid], total[:, hid:]
            hidden = (gate / (1.0 + jnp.exp(-gate)) * up).astype(BF16)
            for k in range(n_ty):
                out_ref[k, keep, :] = hidden

    return kernel(body, ((n_ty, rows, hid),), parts)


def down(where, hidden, w_down, pieces):
    n_ty, rows, _ = hidden.shape
    n_tx = len(pieces) + 1
    half = rows // 2
    width = w_down.shape[-1]

    def body(at_ref, h_ref, wd_ref, *rest):
        piece_refs, out_ref = rest[:-1], rest[-1]
        tx = at_ref[1]
        h = jnp.concatenate([h_ref[k] for k in range(n_ty)], axis=1)
        for d in range(n_tx):
            w = [wd_ref[b, tx] if d == 0 else piece_refs[d - 1][b] for b in range(n_ty)]
            part = dot(h, jnp.concatenate(w, axis=0)).astype(BF16)
            to = lax.rem(tx + (n_tx - d), n_tx)
            out_ref[to] = part[:half]
            out_ref[n_tx + to] = part[half:]

    outs = ((2 * n_tx, half, width),)
    return kernel(body, outs, where, hidden, w_down, *pieces, limit=24)


def join_rows(parts, cap):
    groups, half, width = parts.shape
    n_tx = groups // 2
    block = 8 * cap
    part = block // 2

    def body(p_ref, out_ref):
        order = order_map(cap, block, False)
        for i in range(2 * half // block):
            keep = slice(i * part, (i + 1) * part)
            both = [
                sum(p_ref[core * n_tx + t, keep].astype(F32) for t in range(n_tx)).astype(BF16)
                for core in range(2)
            ]
            out_ref[i * block : (i + 1) * block] = dot(
                order, jnp.concatenate(both, axis=0)
            ).astype(BF16)

    return kernel(body, ((2 * half, width),), parts)


def combine(back, c0, c1, weights, stream):
    def body(back_ref, c0_ref, c1_ref, w_ref, stream_ref, out_ref):
        rows = back_ref[...]
        feed = dot(c0_ref[...], rows) * w_ref[:, 0:1] + dot(c1_ref[...], rows) * w_ref[:, 1:2]
        out_ref[...] = (stream_ref[...].astype(F32) + feed).astype(BF16)

    return kernel(body, (stream.shape,), back, c0, c1, weights, stream)


def shifted(value, axis, steps):
    count = lax.axis_size(axis)
    return lax.ppermute(value, axis, [(i, (i + steps) % count) for i in range(count)])


def local(
    b_gate,
    c_gate,
    h_in,
    docs,
    conv_taps,
    out_weight,
    residual_in,
    norm_gain,
    expert_pick,
    route_weight,
    w_gate,
    w_up,
    w_down,
):
    toks, chans = h_in.shape
    width = residual_in.shape[1]
    full_dim = w_gate.shape[1]
    hid = w_gate.shape[2]
    n_z, n_ty, n_tx = (lax.axis_size(a) for a in ("z", "ty", "tx"))
    n_sp = 2 * n_z
    cap = 5 * toks // (2 * n_sp)
    rows = n_sp * cap
    sp_index = lax.axis_index(("z", "core"))
    ty, tx = lax.axis_index("ty"), lax.axis_index("tx")
    tp_index = ty * n_tx + tx
    where = jnp.stack([ty, tx]).astype(jnp.int32)

    product = (c_gate.astype(F32) * h_in.astype(F32)).astype(BF16)
    edge = lax.ppermute(
        product[toks - 2 :], ("z", "core"), [(i, i + 1) for i in range(n_sp - 1)]
    )
    first_pos = sp_index * toks
    padded_docs = jnp.concatenate([jnp.full((2,), -1, jnp.int32), docs], axis=0)
    near = lax.dynamic_slice_in_dim(padded_docs, first_pos, toks + 2)
    taps = lax.dynamic_slice_in_dim(conv_taps, tp_index * chans, chans, 1).astype(F32)
    extended = jnp.concatenate([edge, product], axis=0).astype(F32)
    conv_sum = taps[0][None, :] * extended[2:]
    for back in (1, 2):
        same = (near[2 - back : 2 - back + toks] == near[2:]).astype(F32)[:, None]
        conv_sum = conv_sum + taps[back][None, :] * extended[2 - back : 2 - back + toks] * same
    conv = (b_gate.astype(F32) * conv_sum).astype(BF16)
    n_tp = n_ty * n_tx
    conv_copies = jnp.broadcast_to(conv.T[None], (n_tp, chans, toks))
    conv_all = lax.all_to_all(conv_copies, TP, 0, 0, tiled=True)
    conv_all = conv_all.reshape(n_tp * chans, toks)

    packed = pack(where, w_gate[0], w_up[0], n_ty)
    gate_up_pieces = [shifted(p, "ty", d + 1) for d, p in enumerate(packed)]
    w_down4 = w_down[0].reshape(n_ty, n_tx, hid, width)
    down_pieces = []
    for d in range(1, n_tx):
        to = lax.rem(tx + d, n_tx)
        piece = lax.dynamic_index_in_dim(w_down4, to, 1, keepdims=False)
        down_pieces.append(shifted(piece, "tx", d))

    ct = routing_out(expert_pick, rows, cap)
    stream, outgoing = project(conv_all, out_weight, residual_in, ct)
    got = lax.all_to_all(
        outgoing.reshape(n_z, 2 * cap, width), "z", 0, 0, tiled=True
    ).reshape(rows, width)
    got, gate_up_pieces = lax.optimization_barrier((got, gate_up_pieces))
    split = split_rows(got, n_tx, cap)
    x = lax.all_to_all(split, ("core", "tx"), 0, 0, tiled=True)
    parts = gate_up(
        where, x, norm_gain.reshape(1, -1), w_gate[0], w_up[0], gate_up_pieces
    )
    parts = lax.all_to_all(parts, "ty", 0, 0, tiled=True)
    hidden = lax.all_to_all(activate(parts, full_dim), "ty", 0, 0, tiled=True)
    outs = lax.all_to_all(
        down(where, hidden, w_down4, down_pieces), ("core", "tx"), 0, 0, tiled=True
    )
    outs, late_pick, late_weight = lax.optimization_barrier((outs, expert_pick, route_weight))
    c0, c1 = routing_back(late_pick, rows, cap)
    back = lax.all_to_all(
        join_rows(outs, cap).reshape(n_z, 2 * cap, width), "z", 0, 0, tiled=True
    ).reshape(rows, width)
    return combine(back, c0, c1, late_weight, stream)


def solution(mesh):
    finer = Mesh(
        mesh.devices.reshape(mesh.shape["sp"] // 2, 2, 4, 4), ("z", "core", "ty", "tx")
    )
    sp = ("z", "core")
    placed = (
        P(sp, TP),
        P(sp, TP),
        P(sp, TP),
        P(),
        P(),
        P(None, TP),
        P(sp, TP),
        P(),
        P(sp, None),
        P(sp, None),
        P(sp, None, TP),
        P(sp, None, TP),
        P(sp, None, TP),
    )

    return jax.shard_map(local, mesh=finer, in_specs=placed, out_specs=P(sp, TP), check_vma=False)
```

```python
import jax
import jax.numpy as jnp
from jax import lax
from jax.experimental import pallas as pl
from jax.experimental.pallas import tpu as pltpu
from jax.sharding import Mesh
from jax.sharding import PartitionSpec as P

TP = ("ty", "tx")
NORM_EPS = 1e-06
F32 = jnp.float32
BF16 = jnp.bfloat16


def dot(a, b, ca=1, cb=0):
    return lax.dot_general(a, b, (((ca,), (cb,)), ((), ())), preferred_element_type=F32)


def kernel(body, outs, *args, limit=12, dtype=BF16):
    vmem = pl.BlockSpec(memory_space=pltpu.VMEM)
    got = pl.pallas_call(
        body,
        out_shape=tuple(jax.ShapeDtypeStruct(o, dtype) for o in outs),
        in_specs=[vmem for a in args],
        out_specs=tuple(vmem for o in outs),
        compiler_params=pltpu.CompilerParams(vmem_limit_bytes=limit << 20 if limit else None),
    )(*args)
    return got if len(outs) > 1 else got[0]


def iota(shape, dim):
    return lax.broadcasted_iota(jnp.int32, shape, dim)


def to_row(col, width, offset):
    rows = col.shape[0]
    hit = iota((rows, width), 0) == iota((rows, width), 1) + offset
    return jnp.sum(jnp.where(hit, col, jnp.zeros((), col.dtype)), axis=0, keepdims=True)


def to_col(row, rows, offset):
    width = row.shape[1]
    hit = iota((rows, width), 0) == iota((rows, width), 1) + offset
    return jnp.sum(jnp.where(hit, row, jnp.zeros((), row.dtype)), axis=1, keepdims=True)


def slots(pick_ref, cap):
    toks = pick_ref.shape[0]
    e0 = pick_ref[:, 0:1]
    e1 = pick_ref[:, 1:2]
    experts = iota((toks, 128), 1)
    oh0 = (experts == e0).astype(F32)
    oh1 = (experts == e1).astype(F32)
    earlier = (iota((toks, toks), 0) > iota((toks, toks), 1)).astype(F32).astype(BF16)
    count = dot(earlier, (oh0 + oh1).astype(BF16))
    s0 = jnp.sum(count * oh0, axis=1, keepdims=True).astype(jnp.int32)
    s1 = jnp.sum((count + oh0) * oh1, axis=1, keepdims=True).astype(jnp.int32)
    return jnp.where(s0 < cap, e0 * cap + s0, -1), jnp.where(s1 < cap, e1 * cap + s1, -1)


def routing_out(pick, cap):
    toks = pick.shape[0]

    def body(pick_ref, out_ref):
        t0, t1 = slots(pick_ref, cap)
        place = iota((8, toks), 0)
        out_ref[...] = jnp.where(place == 0, to_row(t0, toks, 0), to_row(t1, toks, 0))

    return kernel(body, ((8, toks),), pick, dtype=jnp.int32)


def routing_back(pick, rows, cap):
    toks = pick.shape[0]

    def body(pick_ref, c0_ref, c1_ref):
        t0, t1 = slots(pick_ref, cap)
        lanes = iota((toks, rows), 1)
        c0_ref[...] = (lanes == t0).astype(F32).astype(BF16)
        c1_ref[...] = (lanes == t1).astype(F32).astype(BF16)

    return kernel(body, ((toks, rows), (toks, rows)), pick)


def project(conv_all, out_weight, residual, slot_rows, rows):
    toks, width = residual.shape

    def body(conv_ref, w_ref, res_ref, slot_ref, stream_ref, out_ref):
        stream = (res_ref[...].astype(F32) + dot(conv_ref[...], w_ref[...], 0, 0)).astype(BF16)
        stream_ref[...] = stream
        across = iota((rows, toks), 0)
        hit = jnp.logical_or(across == slot_ref[0:1, :], across == slot_ref[1:2, :])
        out_ref[...] = dot(hit.astype(F32).astype(BF16), stream).astype(BF16)

    outs = ((toks, width), (rows, width))
    return kernel(body, outs, conv_all, out_weight, residual, slot_rows)


def convolve(b_gate, c_gate, h_in, edge, same, taps, copies):
    chans, toks = h_in.shape

    def body(b_ref, c_ref, h_ref, edge_ref, same_ref, taps_ref, out_ref):
        product = (c_ref[...].astype(F32) * h_ref[...].astype(F32)).astype(BF16).astype(F32)
        lanes = iota((chans, toks), 1)
        before = [edge_ref[:, k : k + 1].astype(F32) for k in range(2)]
        tap = [to_col(taps_ref[k : k + 1, :], chans, 0) for k in range(3)]
        one = jnp.where(lanes == 0, before[1], pltpu.roll(product, 1, 1))
        two = pltpu.roll(product, 2, 1)
        two = jnp.where(lanes == 0, before[0], jnp.where(lanes == 1, before[1], two))
        total = tap[0] * product
        total = total + tap[1] * one * same_ref[0:1, :]
        total = total + tap[2] * two * same_ref[1:2, :]
        conv = (b_ref[...].astype(F32) * total).astype(BF16)
        for k in range(copies):
            out_ref[k] = conv

    outs = ((copies, chans, toks),)
    return kernel(body, outs, b_gate, c_gate, h_in, edge, same, taps, limit=None)


def order_map(cap, block, splitting):
    q = iota((block, 1), 0)
    if splitting:
        core = (q >= block // 2).astype(jnp.int32)
        within = q - core * (block // 2)
        z = (within * (65536 // cap + 1)) >> 16
        source = within + z * cap + core * cap
    else:
        z = (q * (65536 // (2 * cap) + 1)) >> 16
        rest = q - z * (2 * cap)
        core = (rest >= cap).astype(jnp.int32)
        source = core * (block // 2) + z * cap + rest - core * cap
    return (iota((block, block), 1) == source).astype(F32).astype(BF16)


def split_rows(got, n_tx, cap):
    rows, width = got.shape
    half = rows // 2
    block = 8 * cap
    part = block // 2

    def body(got_ref, out_ref):
        order = order_map(cap, block, True)
        for i in range(rows // block):
            both = dot(order, got_ref[i * block : (i + 1) * block]).astype(BF16)
            for core in range(2):
                for t in range(n_tx):
                    out_ref[core * n_tx + t, i * part : (i + 1) * part] = both[
                        core * part : (core + 1) * part
                    ]

    return kernel(body, ((2 * n_tx, half, width),), got)


def pack(w_gate, w_up, n_ty, steps):
    dim, hid = w_gate.shape
    feats = dim // n_ty

    def body(wg_ref, wu_ref, *out_refs):
        ty = lax.axis_index("ty")
        for d, out_ref in zip(steps, out_refs):
            to = lax.rem(ty + d, n_ty)
            rows = pl.ds(pl.multiple_of(to * feats, feats), feats)
            out_ref[:, :hid] = wg_ref[rows, :]
            out_ref[:, hid:] = wu_ref[rows, :]

    outs = tuple((feats, 2 * hid) for d in steps)
    return kernel(body, outs, w_gate, w_up)


def gate_up(x, gain, w_gate, w_up, pieces):
    n_ty = len(pieces) + 1
    groups, half, width = x.shape
    n_tx = groups // 2
    feats = n_tx * width
    hid = w_gate.shape[1]
    rows = 2 * half

    def body(x_ref, gain_ref, wg_ref, wu_ref, *rest):
        piece_refs, out_ref = rest[:-1], rest[-1]
        ty = lax.axis_index("ty")
        mine = pl.ds(pl.multiple_of(ty * feats, feats), feats)
        gain_row = gain_ref[:, mine].astype(F32)
        extra = jnp.zeros((8, 2 * hid), F32)
        place = iota((8, 2 * hid), 0)
        for core in range(2):
            raw = jnp.concatenate([x_ref[core * n_tx + t] for t in range(n_tx)], axis=1).astype(F32)
            squares = jnp.sum(raw * raw, axis=1, keepdims=True)
            y = (raw * gain_row).astype(BF16)
            for k in range(2):
                row = to_row(squares, 2 * hid, k * 2 * hid)
                high = row.astype(BF16).astype(F32)
                at = core * 2 + k
                extra = jnp.where(place == at, high, extra)
                extra = jnp.where(place == at + 4, row - high, extra)
            keep = slice(core * half, (core + 1) * half)
            out_ref[ty, keep, 0:hid] = dot(y, wg_ref[mine, :]).astype(BF16)
            out_ref[ty, keep, hid : 2 * hid] = dot(y, wu_ref[mine, :]).astype(BF16)
            for d in range(1, n_ty):
                to = lax.rem(ty + (n_ty - d), n_ty)
                out_ref[to, keep, :] = dot(y, piece_refs[d - 1][...]).astype(BF16)
        for to in range(n_ty):
            out_ref[to, rows : rows + 8, :] = extra.astype(BF16)

    outs = ((n_ty, rows + 8, 2 * hid),)
    return kernel(body, outs, x, gain, w_gate, w_up, *pieces, limit=24)


def activate(parts, full_dim):
    n_ty, padded, both = parts.shape
    rows, hid = padded - 8, both // 2
    half = rows // 2

    def body(p_ref, out_ref):
        extra = sum(p_ref[k, rows : rows + 8, :].astype(F32) for k in range(n_ty))
        for core in range(2):
            keep = slice(core * half, (core + 1) * half)
            total = sum(p_ref[k, keep, :].astype(F32) for k in range(n_ty))
            squares = jnp.zeros((half, 1), F32)
            for k in range(2):
                at = core * 2 + k
                row = extra[at : at + 1] + extra[at + 4 : at + 5]
                squares = squares + to_col(row, half, k * both)
            total = total * lax.rsqrt(squares / full_dim + NORM_EPS)
            gate, up = total[:, :hid], total[:, hid:]
            hidden = (gate / (1.0 + jnp.exp(-gate)) * up).astype(BF16)
            for k in range(n_ty):
                out_ref[k, keep, :] = hidden

    return kernel(body, ((n_ty, rows, hid),), parts)


def down(hidden, w_down, pieces):
    n_ty, rows, _ = hidden.shape
    n_tx = len(pieces) + 1
    half = rows // 2
    width = w_down.shape[-1]

    def body(h_ref, wd_ref, *rest):
        piece_refs, out_ref = rest[:-1], rest[-1]
        tx = lax.axis_index("tx")
        h = jnp.concatenate([h_ref[k] for k in range(n_ty)], axis=1)
        for d in range(n_tx):
            w = [wd_ref[b, tx] if d == 0 else piece_refs[d - 1][b] for b in range(n_ty)]
            part = dot(h, jnp.concatenate(w, axis=0)).astype(BF16)
            to = lax.rem(tx + (n_tx - d), n_tx)
            out_ref[to] = part[:half]
            out_ref[n_tx + to] = part[half:]

    outs = ((2 * n_tx, half, width),)
    return kernel(body, outs, hidden, w_down, *pieces, limit=24)


def join_rows(parts, cap):
    groups, half, width = parts.shape
    n_tx = groups // 2
    block = 8 * cap
    part = block // 2

    def body(p_ref, out_ref):
        order = order_map(cap, block, False)
        for i in range(2 * half // block):
            keep = slice(i * part, (i + 1) * part)
            both = [
                sum(p_ref[core * n_tx + t, keep].astype(F32) for t in range(n_tx)).astype(BF16)
                for core in range(2)
            ]
            out_ref[i * block : (i + 1) * block] = dot(
                order, jnp.concatenate(both, axis=0)
            ).astype(BF16)

    return kernel(body, ((2 * half, width),), parts)


def combine(back, c0, c1, weights, stream):
    def body(back_ref, c0_ref, c1_ref, w_ref, stream_ref, out_ref):
        rows = back_ref[...]
        feed = dot(c0_ref[...], rows) * w_ref[:, 0:1] + dot(c1_ref[...], rows) * w_ref[:, 1:2]
        out_ref[...] = (stream_ref[...].astype(F32) + feed).astype(BF16)

    return kernel(body, (stream.shape,), back, c0, c1, weights, stream)


def shifted(value, axis, steps):
    count = lax.axis_size(axis)
    return lax.ppermute(value, axis, [(i, (i + steps) % count) for i in range(count)])


def local(
    b_gate,
    c_gate,
    h_in,
    docs,
    conv_taps,
    out_weight,
    residual_in,
    norm_gain,
    expert_pick,
    route_weight,
    w_gate,
    w_up,
    w_down,
):
    toks, chans = h_in.shape
    width = residual_in.shape[1]
    full_dim = w_gate.shape[1]
    hid = w_gate.shape[2]
    n_z, n_ty, n_tx = (lax.axis_size(a) for a in ("z", "ty", "tx"))
    n_sp = 2 * n_z
    cap = 5 * toks // (2 * n_sp)
    rows = n_sp * cap
    sp_index = lax.axis_index(("z", "core"))
    ty, tx = lax.axis_index("ty"), lax.axis_index("tx")
    tp_index = ty * n_tx + tx

    last = slice(toks - 2, toks)
    product = (c_gate[last].astype(F32) * h_in[last].astype(F32)).astype(BF16)
    edge = lax.ppermute(product, ("z", "core"), [(i, i + 1) for i in range(n_sp - 1)])
    first_pos = sp_index * toks
    padded_docs = jnp.concatenate([jnp.full((2,), -1, jnp.int32), docs], axis=0)
    near = lax.dynamic_slice_in_dim(padded_docs, first_pos, toks + 2)
    same = jnp.stack([near[1 : toks + 1], near[:toks]]) == near[None, 2:]
    taps = lax.dynamic_slice_in_dim(conv_taps, tp_index * chans, chans, 1).astype(F32)
    n_tp = n_ty * n_tx
    conv_copies = convolve(b_gate.T, c_gate.T, h_in.T, edge.T, same.astype(F32), taps, n_tp)
    conv_all = lax.all_to_all(conv_copies, TP, 0, 0, tiled=True)
    conv_all = conv_all.reshape(n_tp * chans, toks)

    first = pack(w_gate[0], w_up[0], n_ty, (1, 2))
    last = pack(w_gate[0], w_up[0], n_ty, (3,))
    gate_up_pieces = [shifted(p, "ty", d + 1) for d, p in enumerate(first)]
    gate_up_pieces.append(shifted(last, "ty", 3))
    w_down4 = w_down[0].reshape(n_ty, n_tx, hid, width)
    down_pieces = []
    for d in range(1, n_tx):
        to = lax.rem(tx + d, n_tx)
        piece = lax.dynamic_index_in_dim(w_down4, to, 1, keepdims=False)
        down_pieces.append(shifted(piece, "tx", d))

    slot_rows = routing_out(expert_pick, cap)
    stream, outgoing = project(conv_all, out_weight, residual_in, slot_rows, rows)
    got = lax.all_to_all(
        outgoing.reshape(n_z, 2 * cap, width), "z", 0, 0, tiled=True
    ).reshape(rows, width)
    split = split_rows(got, n_tx, cap)
    x = lax.all_to_all(split, ("core", "tx"), 0, 0, tiled=True)
    parts = gate_up(
        x, norm_gain.reshape(1, -1), w_gate[0], w_up[0], gate_up_pieces
    )
    parts = lax.all_to_all(parts, "ty", 0, 0, tiled=True)
    hidden = activate(parts, full_dim)
    hidden = lax.all_to_all(hidden, "ty", 0, 0, tiled=True)
    outs = lax.all_to_all(
        down(hidden, w_down4, down_pieces), ("core", "tx"), 0, 0, tiled=True
    )
    outs, late_pick, late_weight = lax.optimization_barrier((outs, expert_pick, route_weight))
    c0, c1 = routing_back(late_pick, rows, cap)
    back = lax.all_to_all(
        join_rows(outs, cap).reshape(n_z, 2 * cap, width), "z", 0, 0, tiled=True
    ).reshape(rows, width)
    return combine(back, c0, c1, late_weight, stream)


def solution(mesh):
    finer = Mesh(
        mesh.devices.reshape(mesh.shape["sp"] // 2, 2, 4, 4), ("z", "core", "ty", "tx")
    )
    sp = ("z", "core")
    placed = (
        P(sp, TP),
        P(sp, TP),
        P(sp, TP),
        P(),
        P(),
        P(None, TP),
        P(sp, TP),
        P(),
        P(sp, None),
        P(sp, None),
        P(sp, None, TP),
        P(sp, None, TP),
        P(sp, None, TP),
    )

    return jax.shard_map(local, mesh=finer, in_specs=placed, out_specs=P(sp, TP), check_vma=False)
```

```python
import jax
import jax.numpy as jnp
from jax import lax
from jax.experimental import pallas as pl
from jax.experimental.pallas import tpu as pltpu
from jax.sharding import Mesh
from jax.sharding import PartitionSpec as P

TP = ("ty", "tx")
NORM_EPS = 1e-06
F32 = jnp.float32
BF16 = jnp.bfloat16


def dot(a, b, ca=1, cb=0):
    return lax.dot_general(a, b, (((ca,), (cb,)), ((), ())), preferred_element_type=F32)


def kernel(body, outs, *args, limit=12, dtype=BF16):
    vmem = pl.BlockSpec(memory_space=pltpu.VMEM)
    got = pl.pallas_call(
        body,
        out_shape=tuple(jax.ShapeDtypeStruct(o, dtype) for o in outs),
        in_specs=[vmem for a in args],
        out_specs=tuple(vmem for o in outs),
        compiler_params=pltpu.CompilerParams(vmem_limit_bytes=limit << 20 if limit else None),
    )(*args)
    return got if len(outs) > 1 else got[0]


def iota(shape, dim):
    return lax.broadcasted_iota(jnp.int32, shape, dim)


def to_row(col, width, offset):
    rows = col.shape[0]
    hit = iota((rows, width), 0) == iota((rows, width), 1) + offset
    return jnp.sum(jnp.where(hit, col, jnp.zeros((), col.dtype)), axis=0, keepdims=True)


def to_col(row, rows, offset):
    width = row.shape[1]
    hit = iota((rows, width), 0) == iota((rows, width), 1) + offset
    return jnp.sum(jnp.where(hit, row, jnp.zeros((), row.dtype)), axis=1, keepdims=True)


def slots(pick_ref, cap):
    toks = pick_ref.shape[0]
    e0 = pick_ref[:, 0:1]
    e1 = pick_ref[:, 1:2]
    experts = iota((toks, 128), 1)
    oh0 = (experts == e0).astype(F32)
    oh1 = (experts == e1).astype(F32)
    earlier = (iota((toks, toks), 0) > iota((toks, toks), 1)).astype(F32).astype(BF16)
    count = dot(earlier, (oh0 + oh1).astype(BF16))
    s0 = jnp.sum(count * oh0, axis=1, keepdims=True).astype(jnp.int32)
    s1 = jnp.sum((count + oh0) * oh1, axis=1, keepdims=True).astype(jnp.int32)
    return jnp.where(s0 < cap, e0 * cap + s0, -1), jnp.where(s1 < cap, e1 * cap + s1, -1)


def routing_out(pick, cap):
    toks = pick.shape[0]

    def body(pick_ref, out_ref):
        t0, t1 = slots(pick_ref, cap)
        place = iota((8, toks), 0)
        out_ref[...] = jnp.where(place == 0, to_row(t0, toks, 0), to_row(t1, toks, 0))

    return kernel(body, ((8, toks),), pick, dtype=jnp.int32)


def routing_back(pick, rows, cap):
    toks = pick.shape[0]

    def body(pick_ref, c0_ref, c1_ref):
        t0, t1 = slots(pick_ref, cap)
        lanes = iota((toks, rows), 1)
        c0_ref[...] = (lanes == t0).astype(F32).astype(BF16)
        c1_ref[...] = (lanes == t1).astype(F32).astype(BF16)

    return kernel(body, ((toks, rows), (toks, rows)), pick)


def project(conv_all, out_weight, residual, slot_rows, rows):
    toks, width = residual.shape

    def body(conv_ref, w_ref, res_ref, slot_ref, stream_ref, out_ref):
        stream = (res_ref[...].astype(F32) + dot(conv_ref[...], w_ref[...], 0, 0)).astype(BF16)
        stream_ref[...] = stream
        across = iota((rows, toks), 0)
        hit = jnp.logical_or(across == slot_ref[0:1, :], across == slot_ref[1:2, :])
        out_ref[...] = dot(hit.astype(F32).astype(BF16), stream).astype(BF16)

    outs = ((toks, width), (rows, width))
    return kernel(body, outs, conv_all, out_weight, residual, slot_rows)


def convolve(b_gate, c_gate, h_in, edge, docs, taps, copies):
    chans, toks = h_in.shape
    lane = docs.shape[1]
    per = toks // lane

    def body(b_ref, c_ref, h_ref, edge_ref, docs_ref, taps_ref, out_ref):
        sp = lax.axis_index("z") * 2 + lax.axis_index("core")
        tp = lax.axis_index("ty") * lax.axis_size("tx") + lax.axis_index("tx")
        own = jnp.concatenate([docs_ref[pl.ds(sp * per + k, 1), :] for k in range(per)], axis=1)
        prior = docs_ref[pl.ds(jnp.maximum(sp * per - 1, 0), 1), :]
        prior = jnp.where(sp > 0, prior, -1)
        at = iota((1, toks), 1)
        back1 = jnp.where(at == 0, prior[:, lane - 1 :], pltpu.roll(own, 1, 1))
        back2 = jnp.where(at == 1, prior[:, lane - 1 :], pltpu.roll(own, 2, 1))
        back2 = jnp.where(at == 0, prior[:, lane - 2 : lane - 1], back2)
        all_taps = taps_ref[...].astype(F32)
        first = lax.rem(all_taps.shape[1] - tp * chans, all_taps.shape[1])
        near = pltpu.roll(jnp.concatenate([all_taps, jnp.zeros((5, all_taps.shape[1]), F32)]), first, 1)
        tap = [to_col(near[k : k + 1, :chans], chans, 0) for k in range(3)]
        product = (c_ref[...].astype(F32) * h_ref[...].astype(F32)).astype(BF16).astype(F32)
        lanes = iota((chans, toks), 1)
        before = [edge_ref[:, k : k + 1].astype(F32) for k in range(2)]
        one = jnp.where(lanes == 0, before[1], pltpu.roll(product, 1, 1))
        two = pltpu.roll(product, 2, 1)
        two = jnp.where(lanes == 0, before[0], jnp.where(lanes == 1, before[1], two))
        total = tap[0] * product
        total = total + tap[1] * one * (back1 == own).astype(F32)
        total = total + tap[2] * two * (back2 == own).astype(F32)
        conv = (b_ref[...].astype(F32) * total).astype(BF16)
        for k in range(copies):
            out_ref[k] = conv

    outs = ((copies, chans, toks),)
    return kernel(body, outs, b_gate, c_gate, h_in, edge, docs, taps, limit=None)


def order_map(cap, block, splitting):
    q = iota((block, 1), 0)
    if splitting:
        core = (q >= block // 2).astype(jnp.int32)
        within = q - core * (block // 2)
        z = (within * (65536 // cap + 1)) >> 16
        source = within + z * cap + core * cap
    else:
        z = (q * (65536 // (2 * cap) + 1)) >> 16
        rest = q - z * (2 * cap)
        core = (rest >= cap).astype(jnp.int32)
        source = core * (block // 2) + z * cap + rest - core * cap
    return (iota((block, block), 1) == source).astype(F32).astype(BF16)


def split_rows(got, n_tx, cap):
    rows, width = got.shape
    half = rows // 2
    block = 8 * cap
    part = block // 2

    def body(got_ref, out_ref):
        order = order_map(cap, block, True)
        for i in range(rows // block):
            both = dot(order, got_ref[i * block : (i + 1) * block]).astype(BF16)
            for core in range(2):
                for t in range(n_tx):
                    out_ref[core * n_tx + t, i * part : (i + 1) * part] = both[
                        core * part : (core + 1) * part
                    ]

    return kernel(body, ((2 * n_tx, half, width),), got)


def pack(w_gate, w_up, n_ty, steps):
    dim, hid = w_gate.shape
    feats = dim // n_ty

    def body(wg_ref, wu_ref, *out_refs):
        ty = lax.axis_index("ty")
        for d, out_ref in zip(steps, out_refs):
            to = lax.rem(ty + d, n_ty)
            rows = pl.ds(pl.multiple_of(to * feats, feats), feats)
            out_ref[:, :hid] = wg_ref[rows, :]
            out_ref[:, hid:] = wu_ref[rows, :]

    outs = tuple((feats, 2 * hid) for d in steps)
    return kernel(body, outs, w_gate, w_up)


def gate_up(x, gain, w_gate, w_up, pieces):
    n_ty = len(pieces) + 1
    groups, half, width = x.shape
    n_tx = groups // 2
    feats = n_tx * width
    hid = w_gate.shape[1]
    rows = 2 * half

    def body(x_ref, gain_ref, wg_ref, wu_ref, *rest):
        piece_refs, out_ref, held, sems = rest[: n_ty - 1], rest[-3], rest[-2], rest[-1]
        moves = [
            pltpu.make_async_copy(ref, held.at[d], sems.at[d]) for d, ref in enumerate(piece_refs)
        ]
        for move in moves:
            move.start()
        ty = lax.axis_index("ty")
        mine = pl.ds(pl.multiple_of(ty * feats, feats), feats)
        gain_row = gain_ref[:, mine].astype(F32)
        extra = jnp.zeros((8, 2 * hid), F32)
        place = iota((8, 2 * hid), 0)
        scaled = []
        for core in range(2):
            raw = jnp.concatenate([x_ref[core * n_tx + t] for t in range(n_tx)], axis=1).astype(F32)
            squares = jnp.sum(raw * raw, axis=1, keepdims=True)
            y = (raw * gain_row).astype(BF16)
            for k in range(2):
                row = to_row(squares, 2 * hid, k * 2 * hid)
                high = row.astype(BF16).astype(F32)
                at = core * 2 + k
                extra = jnp.where(place == at, high, extra)
                extra = jnp.where(place == at + 4, row - high, extra)
            keep = slice(core * half, (core + 1) * half)
            out_ref[ty, keep, 0:hid] = dot(y, wg_ref[mine, :]).astype(BF16)
            out_ref[ty, keep, hid : 2 * hid] = dot(y, wu_ref[mine, :]).astype(BF16)
            scaled.append(y)
        for d in range(1, n_ty):
            to = lax.rem(ty + (n_ty - d), n_ty)
            moves[d - 1].wait()
            for core in range(2):
                keep = slice(core * half, (core + 1) * half)
                out_ref[to, keep, :] = dot(scaled[core], held[d - 1]).astype(BF16)
        for to in range(n_ty):
            out_ref[to, rows : rows + 8, :] = extra.astype(BF16)

    vmem = pl.BlockSpec(memory_space=pltpu.VMEM)
    anywhere = pl.BlockSpec(memory_space=pltpu.HBM)
    return pl.pallas_call(
        body,
        out_shape=jax.ShapeDtypeStruct((n_ty, rows + 8, 2 * hid), BF16),
        in_specs=[vmem] * 4 + [anywhere] * (n_ty - 1),
        out_specs=vmem,
        scratch_shapes=[
            pltpu.VMEM((n_ty - 1, feats, 2 * hid), BF16),
            pltpu.SemaphoreType.DMA((n_ty - 1,)),
        ],
        compiler_params=pltpu.CompilerParams(vmem_limit_bytes=24 << 20),
        name="gate_up",
    )(x, gain, w_gate, w_up, *[pltpu.with_memory_space_constraint(p, pltpu.HBM) for p in pieces])


def activate(parts, full_dim):
    n_ty, padded, both = parts.shape
    rows, hid = padded - 8, both // 2
    half = rows // 2

    def body(p_ref, out_ref):
        extra = sum(p_ref[k, rows : rows + 8, :].astype(F32) for k in range(n_ty))
        for core in range(2):
            keep = slice(core * half, (core + 1) * half)
            total = sum(p_ref[k, keep, :].astype(F32) for k in range(n_ty))
            squares = jnp.zeros((half, 1), F32)
            for k in range(2):
                at = core * 2 + k
                row = extra[at : at + 1] + extra[at + 4 : at + 5]
                squares = squares + to_col(row, half, k * both)
            total = total * lax.rsqrt(squares / full_dim + NORM_EPS)
            gate, up = total[:, :hid], total[:, hid:]
            hidden = (gate / (1.0 + jnp.exp(-gate)) * up).astype(BF16)
            for k in range(n_ty):
                out_ref[k, keep, :] = hidden

    return kernel(body, ((n_ty, rows, hid),), parts)


def down(hidden, w_down, pieces):
    n_ty, rows, _ = hidden.shape
    n_tx = len(pieces) + 1
    half = rows // 2
    width = w_down.shape[-1]

    def body(h_ref, wd_ref, *rest):
        piece_refs, out_ref = rest[:-1], rest[-1]
        tx = lax.axis_index("tx")
        h = jnp.concatenate([h_ref[k] for k in range(n_ty)], axis=1)
        for d in range(n_tx):
            w = [wd_ref[b, tx] if d == 0 else piece_refs[d - 1][b] for b in range(n_ty)]
            part = dot(h, jnp.concatenate(w, axis=0)).astype(BF16)
            to = lax.rem(tx + (n_tx - d), n_tx)
            out_ref[to] = part[:half]
            out_ref[n_tx + to] = part[half:]

    outs = ((2 * n_tx, half, width),)
    return kernel(body, outs, hidden, w_down, *pieces, limit=24)


def join_rows(parts, cap):
    groups, half, width = parts.shape
    n_tx = groups // 2
    block = 8 * cap
    part = block // 2

    def body(p_ref, out_ref):
        order = order_map(cap, block, False)
        for i in range(2 * half // block):
            keep = slice(i * part, (i + 1) * part)
            both = [
                sum(p_ref[core * n_tx + t, keep].astype(F32) for t in range(n_tx)).astype(BF16)
                for core in range(2)
            ]
            out_ref[i * block : (i + 1) * block] = dot(
                order, jnp.concatenate(both, axis=0)
            ).astype(BF16)

    return kernel(body, ((2 * half, width),), parts)


def combine(back, c0, c1, weights, stream):
    def body(back_ref, c0_ref, c1_ref, w_ref, stream_ref, out_ref):
        rows = back_ref[...]
        feed = dot(c0_ref[...], rows) * w_ref[:, 0:1] + dot(c1_ref[...], rows) * w_ref[:, 1:2]
        out_ref[...] = (stream_ref[...].astype(F32) + feed).astype(BF16)

    return kernel(body, (stream.shape,), back, c0, c1, weights, stream)


def shifted(value, axis, steps):
    count = lax.axis_size(axis)
    return lax.ppermute(value, axis, [(i, (i + steps) % count) for i in range(count)])


def local(
    b_gate,
    c_gate,
    h_in,
    docs,
    conv_taps,
    out_weight,
    residual_in,
    norm_gain,
    expert_pick,
    route_weight,
    w_gate,
    w_up,
    w_down,
):
    toks, chans = h_in.shape
    width = residual_in.shape[1]
    full_dim = w_gate.shape[1]
    hid = w_gate.shape[2]
    n_z, n_ty, n_tx = (lax.axis_size(a) for a in ("z", "ty", "tx"))
    n_sp = 2 * n_z
    cap = 5 * toks // (2 * n_sp)
    rows = n_sp * cap
    tx = lax.axis_index("tx")

    last = slice(toks - 2, toks)
    product = (c_gate[last].astype(F32) * h_in[last].astype(F32)).astype(BF16)
    edge = lax.ppermute(product, ("z", "core"), [(i, i + 1) for i in range(n_sp - 1)])
    n_tp = n_ty * n_tx
    conv_copies = convolve(
        b_gate.T, c_gate.T, h_in.T, edge.T, docs.reshape(-1, 128), conv_taps, n_tp
    )
    conv_all = lax.all_to_all(conv_copies, TP, 0, 0, tiled=True)
    conv_all = conv_all.reshape(n_tp * chans, toks)

    first = pack(w_gate[0], w_up[0], n_ty, (1, 2))
    last = pack(w_gate[0], w_up[0], n_ty, (3,))
    gate_up_pieces = [shifted(p, "ty", d + 1) for d, p in enumerate(first)]
    gate_up_pieces.append(shifted(last, "ty", 3))
    w_down4 = w_down[0].reshape(n_ty, n_tx, hid, width)
    down_pieces = []
    for d in range(1, n_tx):
        to = lax.rem(tx + d, n_tx)
        piece = lax.dynamic_index_in_dim(w_down4, to, 1, keepdims=False)
        down_pieces.append(shifted(piece, "tx", d))

    slot_rows = routing_out(expert_pick, cap)
    stream, outgoing = project(conv_all, out_weight, residual_in, slot_rows, rows)
    got = lax.all_to_all(
        outgoing.reshape(n_z, 2 * cap, width), "z", 0, 0, tiled=True
    ).reshape(rows, width)
    split = split_rows(got, n_tx, cap)
    x = lax.all_to_all(split, ("core", "tx"), 0, 0, tiled=True)
    parts = gate_up(x, norm_gain.reshape(1, -1), w_gate[0], w_up[0], gate_up_pieces)
    parts = lax.all_to_all(parts, "ty", 0, 0, tiled=True)
    hidden = activate(parts, full_dim)
    hidden = lax.all_to_all(hidden, "ty", 0, 0, tiled=True)
    outs = lax.all_to_all(
        down(hidden, w_down4, down_pieces), ("core", "tx"), 0, 0, tiled=True
    )
    outs, late_pick, late_weight = lax.optimization_barrier((outs, expert_pick, route_weight))
    c0, c1 = routing_back(late_pick, rows, cap)
    back = lax.all_to_all(
        join_rows(outs, cap).reshape(n_z, 2 * cap, width), "z", 0, 0, tiled=True
    ).reshape(rows, width)
    return combine(back, c0, c1, late_weight, stream)


def solution(mesh):
    finer = Mesh(
        mesh.devices.reshape(mesh.shape["sp"] // 2, 2, 4, 4), ("z", "core", "ty", "tx")
    )
    sp = ("z", "core")
    placed = (
        P(sp, TP),
        P(sp, TP),
        P(sp, TP),
        P(),
        P(),
        P(None, TP),
        P(sp, TP),
        P(),
        P(sp, None),
        P(sp, None),
        P(sp, None, TP),
        P(sp, None, TP),
        P(sp, None, TP),
    )

    return jax.shard_map(local, mesh=finer, in_specs=placed, out_specs=P(sp, TP), check_vma=False)
```

```python
import jax
import jax.numpy as jnp
from jax import lax
from jax.experimental import pallas as pl
from jax.experimental.pallas import tpu as pltpu
from jax.sharding import Mesh
from jax.sharding import PartitionSpec as P

TP = ("ty", "tx")
NORM_EPS = 1e-06
F32 = jnp.float32
BF16 = jnp.bfloat16


def dot(a, b, ca=1, cb=0):
    return lax.dot_general(a, b, (((ca,), (cb,)), ((), ())), preferred_element_type=F32)


def kernel(body, outs, *args, limit=12, dtype=BF16):
    vmem = pl.BlockSpec(memory_space=pltpu.VMEM)
    got = pl.pallas_call(
        body,
        out_shape=tuple(jax.ShapeDtypeStruct(o, dtype) for o in outs),
        in_specs=[vmem for a in args],
        out_specs=tuple(vmem for o in outs),
        compiler_params=pltpu.CompilerParams(vmem_limit_bytes=limit << 20 if limit else None),
    )(*args)
    return got if len(outs) > 1 else got[0]


def iota(shape, dim):
    return lax.broadcasted_iota(jnp.int32, shape, dim)


def to_row(col, width, offset):
    rows = col.shape[0]
    hit = iota((rows, width), 0) == iota((rows, width), 1) + offset
    return jnp.sum(jnp.where(hit, col, jnp.zeros((), col.dtype)), axis=0, keepdims=True)


def to_col(row, rows, offset):
    width = row.shape[1]
    hit = iota((rows, width), 0) == iota((rows, width), 1) + offset
    return jnp.sum(jnp.where(hit, row, jnp.zeros((), row.dtype)), axis=1, keepdims=True)


def slots(pick_ref, cap):
    toks = pick_ref.shape[0]
    e0 = pick_ref[:, 0:1]
    e1 = pick_ref[:, 1:2]
    experts = iota((toks, 128), 1)
    oh0 = (experts == e0).astype(F32)
    oh1 = (experts == e1).astype(F32)
    earlier = (iota((toks, toks), 0) > iota((toks, toks), 1)).astype(F32).astype(BF16)
    count = dot(earlier, (oh0 + oh1).astype(BF16))
    s0 = jnp.sum(count * oh0, axis=1, keepdims=True).astype(jnp.int32)
    s1 = jnp.sum((count + oh0) * oh1, axis=1, keepdims=True).astype(jnp.int32)
    return jnp.where(s0 < cap, e0 * cap + s0, -1), jnp.where(s1 < cap, e1 * cap + s1, -1)


def routing_out(pick, cap):
    toks = pick.shape[0]

    def body(pick_ref, out_ref):
        t0, t1 = slots(pick_ref, cap)
        place = iota((8, toks), 0)
        out_ref[...] = jnp.where(place == 0, to_row(t0, toks, 0), to_row(t1, toks, 0))

    return kernel(body, ((8, toks),), pick, dtype=jnp.int32)


def project(conv_all, out_weight, residual, slot_rows, rows):
    toks, width = residual.shape

    def body(conv_ref, w_ref, res_ref, slot_ref, stream_ref, out_ref):
        stream = (res_ref[...].astype(F32) + dot(conv_ref[...], w_ref[...], 0, 0)).astype(BF16)
        stream_ref[...] = stream
        across = iota((rows, toks), 0)
        hit = jnp.logical_or(across == slot_ref[0:1, :], across == slot_ref[1:2, :])
        out_ref[...] = dot(hit.astype(F32).astype(BF16), stream).astype(BF16)

    outs = ((toks, width), (rows, width))
    return kernel(body, outs, conv_all, out_weight, residual, slot_rows)


def convolve_head(b_gate, c_gate, h_in, docs, taps):
    chans, toks = h_in.shape
    lane = docs.shape[1]
    per = toks // lane

    def body(b_ref, c_ref, h_ref, docs_ref, taps_ref, total_ref, factor_ref, gate_ref):
        gate_ref[...] = b_ref[...].astype(F32)
        sp = lax.axis_index("z") * 2 + lax.axis_index("core")
        tp = lax.axis_index("ty") * lax.axis_size("tx") + lax.axis_index("tx")
        own = jnp.concatenate([docs_ref[pl.ds(sp * per + k, 1), :] for k in range(per)], axis=1)
        prior = docs_ref[pl.ds(jnp.maximum(sp * per - 1, 0), 1), :]
        prior = jnp.where(sp > 0, prior, -1)
        at = iota((1, toks), 1)
        back1 = jnp.where(at == 0, prior[:, lane - 1 :], pltpu.roll(own, 1, 1))
        back2 = jnp.where(at == 1, prior[:, lane - 1 :], pltpu.roll(own, 2, 1))
        back2 = jnp.where(at == 0, prior[:, lane - 2 : lane - 1], back2)
        same1 = (back1 == own).astype(F32)
        same2 = (back2 == own).astype(F32)
        all_taps = taps_ref[...].astype(F32)
        length = all_taps.shape[1]
        first = lax.rem(length - tp * chans, length)
        near = pltpu.roll(jnp.concatenate([all_taps, jnp.zeros((5, length), F32)]), first, 1)
        tap = [to_col(near[k : k + 1, :chans], chans, 0) for k in range(3)]
        product = (c_ref[...].astype(F32) * h_ref[...].astype(F32)).astype(BF16).astype(F32)
        lanes = iota((chans, toks), 1)
        one = jnp.where(lanes >= 1, pltpu.roll(product, 1, 1), 0.0)
        two = jnp.where(lanes >= 2, pltpu.roll(product, 2, 1), 0.0)
        total_ref[...] = tap[0] * product + tap[1] * one * same1 + tap[2] * two * same2
        place = iota((chans, lane), 1)
        factor = jnp.where(place == 0, tap[1] * same1[:, 0:1], tap[2] * same2[:, 0:1])
        factor_ref[...] = jnp.where(place == 2, tap[2] * same2[:, 1:2], factor)

    outs = ((chans, toks), (chans, lane), (chans, toks))
    return kernel(body, outs, b_gate, c_gate, h_in, docs, taps, dtype=F32)


def convolve(total, factor, gate, edge, copies):
    chans, toks = gate.shape

    def body(total_ref, factor_ref, gate_ref, edge_ref, out_ref):
        before = [edge_ref[:, k : k + 1].astype(F32) for k in range(2)]
        at0, at1, at2 = (factor_ref[:, k : k + 1] for k in range(3))
        lanes = iota((chans, toks), 1)
        whole = total_ref[...]
        whole = whole + jnp.where(lanes == 0, at0 * before[1], 0.0)
        whole = whole + jnp.where(
            lanes == 0, at1 * before[0], jnp.where(lanes == 1, at2 * before[1], 0.0)
        )
        conv = (gate_ref[...] * whole).astype(BF16)
        for k in range(copies):
            out_ref[k] = conv

    return kernel(body, ((copies, chans, toks),), total, factor, gate, edge)


def order_map(cap, block, splitting):
    q = iota((block, 1), 0)
    if splitting:
        core = (q >= block // 2).astype(jnp.int32)
        within = q - core * (block // 2)
        z = (within * (65536 // cap + 1)) >> 16
        source = within + z * cap + core * cap
    else:
        z = (q * (65536 // (2 * cap) + 1)) >> 16
        rest = q - z * (2 * cap)
        core = (rest >= cap).astype(jnp.int32)
        source = core * (block // 2) + z * cap + rest - core * cap
    return (iota((block, block), 1) == source).astype(F32).astype(BF16)


def split_rows(got, n_tx, cap):
    rows, width = got.shape
    half = rows // 2
    block = 8 * cap
    part = block // 2

    def body(got_ref, out_ref):
        order = order_map(cap, block, True)
        for i in range(rows // block):
            both = dot(order, got_ref[i * block : (i + 1) * block]).astype(BF16)
            for core in range(2):
                for t in range(n_tx):
                    out_ref[core * n_tx + t, i * part : (i + 1) * part] = both[
                        core * part : (core + 1) * part
                    ]

    return kernel(body, ((2 * n_tx, half, width),), got)


def pack(w_gate, w_up, n_ty, steps):
    dim, hid = w_gate.shape
    feats = dim // n_ty

    def body(wg_ref, wu_ref, *out_refs):
        ty = lax.axis_index("ty")
        for d, out_ref in zip(steps, out_refs):
            to = lax.rem(ty + d, n_ty)
            rows = pl.ds(pl.multiple_of(to * feats, feats), feats)
            out_ref[:, :hid] = wg_ref[rows, :]
            out_ref[:, hid:] = wu_ref[rows, :]

    outs = tuple((feats, 2 * hid) for d in steps)
    return kernel(body, outs, w_gate, w_up)


def gate_up(x, gain, w_gate, w_up, pieces):
    n_ty = len(pieces) + 1
    groups, half, width = x.shape
    n_tx = groups // 2
    feats = n_tx * width
    hid = w_gate.shape[1]
    rows = 2 * half

    def body(x_ref, gain_ref, wg_ref, wu_ref, *rest):
        piece_refs, out_ref, held, sems = rest[: n_ty - 1], rest[-3], rest[-2], rest[-1]
        moves = [
            pltpu.make_async_copy(ref, held.at[d], sems.at[d]) for d, ref in enumerate(piece_refs)
        ]
        for move in moves:
            move.start()
        ty = lax.axis_index("ty")
        mine = pl.ds(pl.multiple_of(ty * feats, feats), feats)
        gain_rows = gain_ref[pl.ds(pl.multiple_of(ty * (feats // 128), 8), feats // 128), :].astype(F32)
        gain_row = jnp.concatenate([gain_rows[k : k + 1] for k in range(feats // 128)], axis=1)
        extra = jnp.zeros((8, 2 * hid), F32)
        place = iota((8, 2 * hid), 0)
        scaled = []
        for core in range(2):
            raw = jnp.concatenate([x_ref[core * n_tx + t] for t in range(n_tx)], axis=1).astype(F32)
            squares = jnp.sum(raw * raw, axis=1, keepdims=True)
            y = (raw * gain_row).astype(BF16)
            for k in range(2):
                row = to_row(squares, 2 * hid, k * 2 * hid)
                high = row.astype(BF16).astype(F32)
                at = core * 2 + k
                extra = jnp.where(place == at, high, extra)
                extra = jnp.where(place == at + 4, row - high, extra)
            keep = slice(core * half, (core + 1) * half)
            out_ref[ty, keep, 0:hid] = dot(y, wg_ref[mine, :]).astype(BF16)
            out_ref[ty, keep, hid : 2 * hid] = dot(y, wu_ref[mine, :]).astype(BF16)
            scaled.append(y)
        for d in range(1, n_ty):
            to = lax.rem(ty + (n_ty - d), n_ty)
            moves[d - 1].wait()
            for core in range(2):
                keep = slice(core * half, (core + 1) * half)
                out_ref[to, keep, :] = dot(scaled[core], held[d - 1]).astype(BF16)
        for to in range(n_ty):
            out_ref[to, rows : rows + 8, :] = extra.astype(BF16)

    vmem = pl.BlockSpec(memory_space=pltpu.VMEM)
    anywhere = pl.BlockSpec(memory_space=pltpu.HBM)
    return pl.pallas_call(
        body,
        out_shape=jax.ShapeDtypeStruct((n_ty, rows + 8, 2 * hid), BF16),
        in_specs=[vmem] * 4 + [anywhere] * (n_ty - 1),
        out_specs=vmem,
        scratch_shapes=[
            pltpu.VMEM((n_ty - 1, feats, 2 * hid), BF16),
            pltpu.SemaphoreType.DMA((n_ty - 1,)),
        ],
        compiler_params=pltpu.CompilerParams(vmem_limit_bytes=24 << 20),
        name="gate_up",
    )(x, gain, w_gate, w_up, *[pltpu.with_memory_space_constraint(p, pltpu.HBM) for p in pieces])


def activate(parts, full_dim):
    n_ty, padded, both = parts.shape
    rows, hid = padded - 8, both // 2
    half = rows // 2

    def body(p_ref, out_ref):
        extra = sum(p_ref[k, rows : rows + 8, :].astype(F32) for k in range(n_ty))
        for core in range(2):
            keep = slice(core * half, (core + 1) * half)
            total = sum(p_ref[k, keep, :].astype(F32) for k in range(n_ty))
            squares = jnp.zeros((half, 1), F32)
            for k in range(2):
                at = core * 2 + k
                row = extra[at : at + 1] + extra[at + 4 : at + 5]
                squares = squares + to_col(row, half, k * both)
            total = total * lax.rsqrt(squares / full_dim + NORM_EPS)
            gate, up = total[:, :hid], total[:, hid:]
            hidden = (gate / (1.0 + jnp.exp(-gate)) * up).astype(BF16)
            for k in range(n_ty):
                out_ref[k, keep, :] = hidden

    return kernel(body, ((n_ty, rows, hid),), parts)


def down(hidden, w_down, pieces):
    n_ty, rows, hid = hidden.shape
    n_tx = len(pieces) + 1
    half = rows // 2
    width = w_down.shape[-1]

    def body(h_ref, wd_ref, *rest):
        piece_refs, out_ref, held, sems = rest[: n_tx - 1], rest[-3], rest[-2], rest[-1]
        moves = [
            pltpu.make_async_copy(ref, held.at[d], sems.at[d]) for d, ref in enumerate(piece_refs)
        ]
        for move in moves:
            move.start()
        tx = lax.axis_index("tx")
        h = jnp.concatenate([h_ref[k] for k in range(n_ty)], axis=1)
        for d in range(n_tx):
            if d:
                moves[d - 1].wait()
            w = [wd_ref[b, tx] if d == 0 else held[d - 1, b] for b in range(n_ty)]
            part = dot(h, jnp.concatenate(w, axis=0)).astype(BF16)
            to = lax.rem(tx + (n_tx - d), n_tx)
            out_ref[to] = part[:half]
            out_ref[n_tx + to] = part[half:]

    vmem = pl.BlockSpec(memory_space=pltpu.VMEM)
    return pl.pallas_call(
        body,
        out_shape=jax.ShapeDtypeStruct((2 * n_tx, half, width), BF16),
        in_specs=[vmem] * 2 + [pl.BlockSpec(memory_space=pltpu.HBM)] * (n_tx - 1),
        out_specs=vmem,
        scratch_shapes=[
            pltpu.VMEM((n_tx - 1, n_ty, hid, width), BF16),
            pltpu.SemaphoreType.DMA((n_tx - 1,)),
        ],
        compiler_params=pltpu.CompilerParams(vmem_limit_bytes=24 << 20),
        name="down",
    )(hidden, w_down, *[pltpu.with_memory_space_constraint(p, pltpu.HBM) for p in pieces])


def join_rows(parts, cap):
    groups, half, width = parts.shape
    n_tx = groups // 2
    block = 8 * cap
    part = block // 2

    def body(p_ref, out_ref):
        order = order_map(cap, block, False)
        for i in range(2 * half // block):
            keep = slice(i * part, (i + 1) * part)
            both = [
                sum(p_ref[core * n_tx + t, keep].astype(F32) for t in range(n_tx)).astype(BF16)
                for core in range(2)
            ]
            out_ref[i * block : (i + 1) * block] = dot(
                order, jnp.concatenate(both, axis=0)
            ).astype(BF16)

    return kernel(body, ((2 * half, width),), parts)


def combine(back, slot_rows, weights, stream):
    toks = stream.shape[0]
    rows = back.shape[0]

    def body(back_ref, slot_ref, w_ref, stream_ref, out_ref):
        got = back_ref[...]
        lanes = iota((toks, rows), 1)
        total = stream_ref[...].astype(F32)
        feed = jnp.zeros(total.shape, F32)
        for k in range(2):
            slot = to_col(slot_ref[k : k + 1, :], toks, 0)
            picked = dot((lanes == slot).astype(F32).astype(BF16), got)
            feed = feed + picked * to_col(w_ref[k : k + 1, :], toks, 0)
        out_ref[...] = (total + feed).astype(BF16)

    return kernel(body, (stream.shape,), back, slot_rows, weights, stream)


def shifted(value, axis, steps):
    count = lax.axis_size(axis)
    return lax.ppermute(value, axis, [(i, (i + steps) % count) for i in range(count)])


def local(
    b_gate,
    c_gate,
    h_in,
    docs,
    conv_taps,
    out_weight,
    residual_in,
    norm_gain,
    expert_pick,
    route_weight,
    w_gate,
    w_up,
    w_down,
):
    toks, chans = h_in.shape
    width = residual_in.shape[1]
    full_dim = w_gate.shape[1]
    hid = w_gate.shape[2]
    n_z, n_ty, n_tx = (lax.axis_size(a) for a in ("z", "ty", "tx"))
    n_sp = 2 * n_z
    cap = 5 * toks // (2 * n_sp)
    rows = n_sp * cap
    tx = lax.axis_index("tx")

    last = slice(toks - 2, toks)
    product = (c_gate[last].astype(F32) * h_in[last].astype(F32)).astype(BF16)
    edge = lax.ppermute(product, ("z", "core"), [(i, i + 1) for i in range(n_sp - 1)])
    n_tp = n_ty * n_tx
    head = convolve_head(b_gate.T, c_gate.T, h_in.T, docs.reshape(-1, 128), conv_taps)
    conv_copies = convolve(*head, edge.T, n_tp)
    conv_all = lax.all_to_all(conv_copies, TP, 0, 0, tiled=True)
    conv_all = conv_all.reshape(n_tp * chans, toks)

    first = pack(w_gate[0], w_up[0], n_ty, (1, 2))
    last = pack(w_gate[0], w_up[0], n_ty, (3,))
    gate_up_pieces = [shifted(p, "ty", d + 1) for d, p in enumerate(first)]
    gate_up_pieces.append(shifted(last, "ty", 3))
    w_down4 = w_down[0].reshape(n_ty, n_tx, hid, width)
    down_pieces = []
    for d in range(1, n_tx):
        to = lax.rem(tx + d, n_tx)
        piece = lax.dynamic_index_in_dim(w_down4, to, 1, keepdims=False)
        down_pieces.append(shifted(piece, "tx", d))

    slot_rows = routing_out(expert_pick, cap)
    stream, outgoing = project(conv_all, out_weight, residual_in, slot_rows, rows)
    got = lax.all_to_all(
        outgoing.reshape(n_z, 2 * cap, width), "z", 0, 0, tiled=True
    ).reshape(rows, width)
    split = split_rows(got, n_tx, cap)
    x = lax.all_to_all(split, ("core", "tx"), 0, 0, tiled=True)
    parts = gate_up(x, norm_gain.reshape(-1, 128), w_gate[0], w_up[0], gate_up_pieces)
    parts = lax.all_to_all(parts, "ty", 0, 0, tiled=True)
    hidden = activate(parts, full_dim)
    hidden = lax.all_to_all(hidden, "ty", 0, 0, tiled=True)
    outs = lax.all_to_all(
        down(hidden, w_down4, down_pieces), ("core", "tx"), 0, 0, tiled=True
    )
    back = lax.all_to_all(
        join_rows(outs, cap).reshape(n_z, 2 * cap, width), "z", 0, 0, tiled=True
    ).reshape(rows, width)
    return combine(back, slot_rows, route_weight.T, stream)


def solution(mesh):
    finer = Mesh(
        mesh.devices.reshape(mesh.shape["sp"] // 2, 2, 4, 4), ("z", "core", "ty", "tx")
    )
    sp = ("z", "core")
    placed = (
        P(sp, TP),
        P(sp, TP),
        P(sp, TP),
        P(),
        P(),
        P(None, TP),
        P(sp, TP),
        P(),
        P(sp, None),
        P(sp, None),
        P(sp, None, TP),
        P(sp, None, TP),
        P(sp, None, TP),
    )

    return jax.shard_map(local, mesh=finer, in_specs=placed, out_specs=P(sp, TP), check_vma=False)
```

```python
import jax
import jax.numpy as jnp
from jax import lax
from jax.experimental import pallas as pl
from jax.experimental.pallas import tpu as pltpu
from jax.sharding import Mesh
from jax.sharding import PartitionSpec as P

TP = ("ty", "tx")
NORM_EPS = 1e-06
F32 = jnp.float32
BF16 = jnp.bfloat16


def dot(a, b, ca=1, cb=0):
    return lax.dot_general(a, b, (((ca,), (cb,)), ((), ())), preferred_element_type=F32)


def kernel(body, outs, *args, limit=12, dtype=BF16):
    vmem = pl.BlockSpec(memory_space=pltpu.VMEM)
    got = pl.pallas_call(
        body,
        out_shape=tuple(jax.ShapeDtypeStruct(o, dtype) for o in outs),
        in_specs=[vmem for a in args],
        out_specs=tuple(vmem for o in outs),
        compiler_params=pltpu.CompilerParams(vmem_limit_bytes=limit << 20 if limit else None),
    )(*args)
    return got if len(outs) > 1 else got[0]


def iota(shape, dim):
    return lax.broadcasted_iota(jnp.int32, shape, dim)


def to_row(col, width, offset):
    rows = col.shape[0]
    hit = iota((rows, width), 0) == iota((rows, width), 1) + offset
    return jnp.sum(jnp.where(hit, col, jnp.zeros((), col.dtype)), axis=0, keepdims=True)


def to_col(row, rows, offset):
    width = row.shape[1]
    hit = iota((rows, width), 0) == iota((rows, width), 1) + offset
    return jnp.sum(jnp.where(hit, row, jnp.zeros((), row.dtype)), axis=1, keepdims=True)


def slots(pick_ref, cap):
    toks = pick_ref.shape[0]
    e0 = pick_ref[:, 0:1]
    e1 = pick_ref[:, 1:2]
    experts = iota((toks, 128), 1)
    oh0 = (experts == e0).astype(F32)
    oh1 = (experts == e1).astype(F32)
    earlier = (iota((toks, toks), 0) > iota((toks, toks), 1)).astype(F32).astype(BF16)
    count = dot(earlier, (oh0 + oh1).astype(BF16))
    s0 = jnp.sum(count * oh0, axis=1, keepdims=True).astype(jnp.int32)
    s1 = jnp.sum((count + oh0) * oh1, axis=1, keepdims=True).astype(jnp.int32)
    return jnp.where(s0 < cap, e0 * cap + s0, -1), jnp.where(s1 < cap, e1 * cap + s1, -1)


def routing_out(pick, cap):
    toks = pick.shape[0]

    def body(pick_ref, out_ref):
        t0, t1 = slots(pick_ref, cap)
        place = iota((8, toks), 0)
        out_ref[...] = jnp.where(place == 0, to_row(t0, toks, 0), to_row(t1, toks, 0))

    return kernel(body, ((8, toks),), pick, dtype=jnp.int32)


def project(conv_all, out_weight, residual, slot_rows, rows):
    toks, width = residual.shape

    def body(conv_ref, w_ref, res_ref, slot_ref, stream_ref, out_ref):
        stream = (res_ref[...].astype(F32) + dot(conv_ref[...], w_ref[...], 0, 0)).astype(BF16)
        stream_ref[...] = stream
        across = iota((rows, toks), 0)
        hit = jnp.logical_or(across == slot_ref[0:1, :], across == slot_ref[1:2, :])
        out_ref[...] = dot(hit.astype(F32).astype(BF16), stream).astype(BF16)

    outs = ((toks, width), (rows, width))
    return kernel(body, outs, conv_all, out_weight, residual, slot_rows)


def convolve_head(b_gate, c_gate, h_in, docs, taps):
    chans, toks = h_in.shape
    lane = docs.shape[1]
    per = toks // lane

    def body(*refs):
        given, (total_ref, factor_ref, gate_ref), held = refs[:5], refs[5:8], refs[8:13]
        moves = [pltpu.make_async_copy(g, k, refs[13].at[i]) for i, (g, k) in enumerate(zip(given, held))]
        for move in moves:
            move.start()
        for move in moves:
            move.wait()
        b_ref, c_ref, h_ref, docs_ref, taps_ref = held
        gate_ref[...] = b_ref[...].astype(F32)
        sp = lax.axis_index("z") * 2 + lax.axis_index("core")
        tp = lax.axis_index("ty") * lax.axis_size("tx") + lax.axis_index("tx")
        own = jnp.concatenate([docs_ref[pl.ds(sp * per + k, 1), :] for k in range(per)], axis=1)
        prior = docs_ref[pl.ds(jnp.maximum(sp * per - 1, 0), 1), :]
        prior = jnp.where(sp > 0, prior, -1)
        at = iota((1, toks), 1)
        back1 = jnp.where(at == 0, prior[:, lane - 1 :], pltpu.roll(own, 1, 1))
        back2 = jnp.where(at == 1, prior[:, lane - 1 :], pltpu.roll(own, 2, 1))
        back2 = jnp.where(at == 0, prior[:, lane - 2 : lane - 1], back2)
        same1 = (back1 == own).astype(F32)
        same2 = (back2 == own).astype(F32)
        all_taps = taps_ref[...].astype(F32)
        length = all_taps.shape[1]
        first = lax.rem(length - tp * chans, length)
        near = pltpu.roll(jnp.concatenate([all_taps, jnp.zeros((5, length), F32)]), first, 1)
        tap = [to_col(near[k : k + 1, :chans], chans, 0) for k in range(3)]
        product = (c_ref[...].astype(F32) * h_ref[...].astype(F32)).astype(BF16).astype(F32)
        lanes = iota((chans, toks), 1)
        one = jnp.where(lanes >= 1, pltpu.roll(product, 1, 1), 0.0)
        two = jnp.where(lanes >= 2, pltpu.roll(product, 2, 1), 0.0)
        total_ref[...] = tap[0] * product + tap[1] * one * same1 + tap[2] * two * same2
        place = iota((chans, lane), 1)
        factor = jnp.where(place == 0, tap[1] * same1[:, 0:1], tap[2] * same2[:, 0:1])
        factor_ref[...] = jnp.where(place == 2, tap[2] * same2[:, 1:2], factor)

    outs = ((chans, toks), (chans, lane), (chans, toks))
    args = (b_gate, c_gate, h_in, docs, taps)
    vmem = pl.BlockSpec(memory_space=pltpu.VMEM)
    return pl.pallas_call(
        body,
        out_shape=tuple(jax.ShapeDtypeStruct(o, F32) for o in outs),
        in_specs=[pl.BlockSpec(memory_space=pltpu.HBM)] * len(args),
        out_specs=(vmem,) * len(outs),
        scratch_shapes=[*[pltpu.VMEM(a.shape, a.dtype) for a in args], pltpu.SemaphoreType.DMA((len(args),))],
        compiler_params=pltpu.CompilerParams(vmem_limit_bytes=12 << 20),
        name="convolve_head",
    )(*[pltpu.with_memory_space_constraint(a, pltpu.HBM) for a in args])


def convolve(total, factor, gate, edge, copies):
    chans, toks = gate.shape

    def body(total_ref, factor_ref, gate_ref, edge_ref, out_ref):
        before = [edge_ref[:, k : k + 1].astype(F32) for k in range(2)]
        at0, at1, at2 = (factor_ref[:, k : k + 1] for k in range(3))
        lanes = iota((chans, toks), 1)
        whole = total_ref[...]
        whole = whole + jnp.where(lanes == 0, at0 * before[1], 0.0)
        whole = whole + jnp.where(
            lanes == 0, at1 * before[0], jnp.where(lanes == 1, at2 * before[1], 0.0)
        )
        conv = (gate_ref[...] * whole).astype(BF16)
        for k in range(copies):
            out_ref[k] = conv

    return kernel(body, ((copies, chans, toks),), total, factor, gate, edge)


def order_map(cap, block, splitting):
    q = iota((block, 1), 0)
    if splitting:
        core = (q >= block // 2).astype(jnp.int32)
        within = q - core * (block // 2)
        z = (within * (65536 // cap + 1)) >> 16
        source = within + z * cap + core * cap
    else:
        z = (q * (65536 // (2 * cap) + 1)) >> 16
        rest = q - z * (2 * cap)
        core = (rest >= cap).astype(jnp.int32)
        source = core * (block // 2) + z * cap + rest - core * cap
    return (iota((block, block), 1) == source).astype(F32).astype(BF16)


def split_rows(got, n_tx, cap):
    rows, width = got.shape
    half = rows // 2
    block = 8 * cap
    part = block // 2

    def body(got_ref, out_ref):
        order = order_map(cap, block, True)
        for i in range(rows // block):
            both = dot(order, got_ref[i * block : (i + 1) * block]).astype(BF16)
            for core in range(2):
                for t in range(n_tx):
                    out_ref[core * n_tx + t, i * part : (i + 1) * part] = both[
                        core * part : (core + 1) * part
                    ]

    return kernel(body, ((2 * n_tx, half, width),), got)


def pack(w_gate, w_up, n_ty, steps):
    dim, hid = w_gate.shape
    feats = dim // n_ty

    def body(wg_ref, wu_ref, *rest):
        out_refs, sems = rest[:-1], rest[-1]
        ty = lax.axis_index("ty")
        moves = []
        for k, d in enumerate(steps):
            to = lax.rem(ty + d, n_ty)
            rows = pl.ds(pl.multiple_of(to * feats, feats), feats)
            for j, w_ref in enumerate((wg_ref, wu_ref)):
                lanes = pl.ds(j * hid, hid)
                moves.append(
                    pltpu.make_async_copy(
                        w_ref.at[rows, :], out_refs[k].at[:, lanes], sems.at[2 * k + j]
                    )
                )
        for move in moves:
            move.start()
        for move in moves:
            move.wait()

    return pl.pallas_call(
        body,
        out_shape=tuple(jax.ShapeDtypeStruct((feats, 2 * hid), BF16) for d in steps),
        in_specs=[pl.BlockSpec(memory_space=pltpu.HBM)] * 2,
        out_specs=tuple(pl.BlockSpec(memory_space=pl.ANY) for d in steps),
        scratch_shapes=[pltpu.SemaphoreType.DMA((2 * len(steps),))],
        compiler_params=pltpu.CompilerParams(vmem_limit_bytes=12 << 20),
    )(*[pltpu.with_memory_space_constraint(w, pltpu.HBM) for w in (w_gate, w_up)])


def gate_up(x, gain, w_gate, w_up, pieces):
    n_ty = len(pieces) + 1
    groups, half, width = x.shape
    n_tx = groups // 2
    feats = n_tx * width
    hid = w_gate.shape[1]
    rows = 2 * half

    def body(x_ref, gain_ref, wg_ref, wu_ref, *rest):
        piece_refs, out_ref, held, sems = rest[: n_ty - 1], rest[-3], rest[-2], rest[-1]
        moves = [
            pltpu.make_async_copy(ref, held.at[d], sems.at[d]) for d, ref in enumerate(piece_refs)
        ]
        for move in moves:
            move.start()
        ty = lax.axis_index("ty")
        mine = pl.ds(pl.multiple_of(ty * feats, feats), feats)
        gain_rows = gain_ref[pl.ds(pl.multiple_of(ty * (feats // 128), 8), feats // 128), :].astype(F32)
        gain_row = jnp.concatenate([gain_rows[k : k + 1] for k in range(feats // 128)], axis=1)
        extra = jnp.zeros((8, 2 * hid), F32)
        place = iota((8, 2 * hid), 0)
        scaled = []
        for core in range(2):
            raw = jnp.concatenate([x_ref[core * n_tx + t] for t in range(n_tx)], axis=1).astype(F32)
            squares = jnp.sum(raw * raw, axis=1, keepdims=True)
            y = (raw * gain_row).astype(BF16)
            for k in range(2):
                row = to_row(squares, 2 * hid, k * 2 * hid)
                high = row.astype(BF16).astype(F32)
                at = core * 2 + k
                extra = jnp.where(place == at, high, extra)
                extra = jnp.where(place == at + 4, row - high, extra)
            keep = slice(core * half, (core + 1) * half)
            out_ref[ty, keep, 0:hid] = dot(y, wg_ref[mine, :]).astype(BF16)
            out_ref[ty, keep, hid : 2 * hid] = dot(y, wu_ref[mine, :]).astype(BF16)
            scaled.append(y)
        for d in range(1, n_ty):
            to = lax.rem(ty + (n_ty - d), n_ty)
            moves[d - 1].wait()
            for core in range(2):
                keep = slice(core * half, (core + 1) * half)
                out_ref[to, keep, :] = dot(scaled[core], held[d - 1]).astype(BF16)
        for to in range(n_ty):
            out_ref[to, rows : rows + 8, :] = extra.astype(BF16)

    vmem = pl.BlockSpec(memory_space=pltpu.VMEM)
    anywhere = pl.BlockSpec(memory_space=pltpu.HBM)
    return pl.pallas_call(
        body,
        out_shape=jax.ShapeDtypeStruct((n_ty, rows + 8, 2 * hid), BF16),
        in_specs=[vmem] * 4 + [anywhere] * (n_ty - 1),
        out_specs=vmem,
        scratch_shapes=[
            pltpu.VMEM((n_ty - 1, feats, 2 * hid), BF16),
            pltpu.SemaphoreType.DMA((n_ty - 1,)),
        ],
        compiler_params=pltpu.CompilerParams(vmem_limit_bytes=24 << 20),
        name="gate_up",
    )(x, gain, w_gate, w_up, *[pltpu.with_memory_space_constraint(p, pltpu.HBM) for p in pieces])


def activate(parts, full_dim):
    n_ty, padded, both = parts.shape
    rows, hid = padded - 8, both // 2
    half = rows // 2

    def body(p_ref, out_ref):
        extra = sum(p_ref[k, rows : rows + 8, :].astype(F32) for k in range(n_ty))
        for core in range(2):
            keep = slice(core * half, (core + 1) * half)
            total = sum(p_ref[k, keep, :].astype(F32) for k in range(n_ty))
            squares = jnp.zeros((half, 1), F32)
            for k in range(2):
                at = core * 2 + k
                row = extra[at : at + 1] + extra[at + 4 : at + 5]
                squares = squares + to_col(row, half, k * both)
            total = total * lax.rsqrt(squares / full_dim + NORM_EPS)
            gate, up = total[:, :hid], total[:, hid:]
            hidden = (gate / (1.0 + jnp.exp(-gate)) * up).astype(BF16)
            for k in range(n_ty):
                out_ref[k, keep, :] = hidden

    return kernel(body, ((n_ty, rows, hid),), parts)


def down(hidden, w_down, pieces):
    n_ty, rows, _ = hidden.shape
    n_tx = len(pieces) + 1
    half = rows // 2
    width = w_down.shape[-1]

    def body(h_ref, wd_ref, *rest):
        piece_refs, out_ref = rest[:-1], rest[-1]
        tx = lax.axis_index("tx")
        h = jnp.concatenate([h_ref[k] for k in range(n_ty)], axis=1)
        for d in range(n_tx):
            w = [wd_ref[b, tx] if d == 0 else piece_refs[d - 1][b] for b in range(n_ty)]
            part = dot(h, jnp.concatenate(w, axis=0)).astype(BF16)
            to = lax.rem(tx + (n_tx - d), n_tx)
            out_ref[to] = part[:half]
            out_ref[n_tx + to] = part[half:]

    outs = ((2 * n_tx, half, width),)
    return kernel(body, outs, hidden, w_down, *pieces, limit=24)


def join_rows(parts, cap):
    groups, half, width = parts.shape
    n_tx = groups // 2
    block = 8 * cap
    part = block // 2

    def body(p_ref, out_ref):
        order = order_map(cap, block, False)
        for i in range(2 * half // block):
            keep = slice(i * part, (i + 1) * part)
            both = [
                sum(p_ref[core * n_tx + t, keep].astype(F32) for t in range(n_tx)).astype(BF16)
                for core in range(2)
            ]
            out_ref[i * block : (i + 1) * block] = dot(
                order, jnp.concatenate(both, axis=0)
            ).astype(BF16)

    return kernel(body, ((2 * half, width),), parts)


def combine(back, slot_rows, weights, stream):
    toks = stream.shape[0]
    rows = back.shape[0]

    def body(back_ref, slot_ref, w_ref, stream_ref, out_ref):
        got = back_ref[...]
        lanes = iota((toks, rows), 1)
        total = stream_ref[...].astype(F32)
        feed = jnp.zeros(total.shape, F32)
        for k in range(2):
            slot = to_col(slot_ref[k : k + 1, :], toks, 0)
            picked = dot((lanes == slot).astype(F32).astype(BF16), got)
            feed = feed + picked * to_col(w_ref[k : k + 1, :], toks, 0)
        out_ref[...] = (total + feed).astype(BF16)

    return kernel(body, (stream.shape,), back, slot_rows, weights, stream)


def shifted(value, axis, steps):
    count = lax.axis_size(axis)
    return lax.ppermute(value, axis, [(i, (i + steps) % count) for i in range(count)])


def local(
    b_gate,
    c_gate,
    h_in,
    docs,
    conv_taps,
    out_weight,
    residual_in,
    norm_gain,
    expert_pick,
    route_weight,
    w_gate,
    w_up,
    w_down,
):
    toks, chans = h_in.shape
    width = residual_in.shape[1]
    full_dim = w_gate.shape[1]
    hid = w_gate.shape[2]
    n_z, n_ty, n_tx = (lax.axis_size(a) for a in ("z", "ty", "tx"))
    n_sp = 2 * n_z
    cap = 5 * toks // (2 * n_sp)
    rows = n_sp * cap
    tx = lax.axis_index("tx")

    last = slice(toks - 2, toks)
    product = (c_gate[last].astype(F32) * h_in[last].astype(F32)).astype(BF16)
    edge = lax.ppermute(product, ("z", "core"), [(i, i + 1) for i in range(n_sp - 1)])
    n_tp = n_ty * n_tx
    head = convolve_head(b_gate.T, c_gate.T, h_in.T, docs.reshape(-1, 128), conv_taps)
    conv_copies = convolve(*head, edge.T, n_tp)
    conv_all = lax.all_to_all(conv_copies, TP, 0, 0, tiled=True)
    conv_all = conv_all.reshape(n_tp * chans, toks)

    first = pack(w_gate[0], w_up[0], n_ty, (1, 2))
    (last,) = pack(w_gate[0], w_up[0], n_ty, (3,))
    gate_up_pieces = [shifted(p, "ty", d + 1) for d, p in enumerate(first)]
    gate_up_pieces.append(shifted(last, "ty", 3))
    w_down4 = w_down[0].reshape(n_ty, n_tx, hid, width)
    down_pieces = []
    for d in range(1, n_tx):
        to = lax.rem(tx + d, n_tx)
        piece = lax.dynamic_index_in_dim(w_down4, to, 1, keepdims=False)
        down_pieces.append(shifted(piece, "tx", d))

    slot_rows = routing_out(expert_pick, cap)
    stream, outgoing = project(conv_all, out_weight, residual_in, slot_rows, rows)
    got = lax.all_to_all(
        outgoing.reshape(n_z, 2 * cap, width), "z", 0, 0, tiled=True
    ).reshape(rows, width)
    split = split_rows(got, n_tx, cap)
    x = lax.all_to_all(split, ("core", "tx"), 0, 0, tiled=True)
    parts = gate_up(x, norm_gain.reshape(-1, 128), w_gate[0], w_up[0], gate_up_pieces)
    parts = lax.all_to_all(parts, "ty", 0, 0, tiled=True)
    hidden = activate(parts, full_dim)
    hidden = lax.all_to_all(hidden, "ty", 0, 0, tiled=True)
    outs = lax.all_to_all(
        down(hidden, w_down4, down_pieces), ("core", "tx"), 0, 0, tiled=True
    )
    back = lax.all_to_all(
        join_rows(outs, cap).reshape(n_z, 2 * cap, width), "z", 0, 0, tiled=True
    ).reshape(rows, width)
    return combine(back, slot_rows, route_weight.T, stream)


def solution(mesh):
    finer = Mesh(
        mesh.devices.reshape(mesh.shape["sp"] // 2, 2, 4, 4), ("z", "core", "ty", "tx")
    )
    sp = ("z", "core")
    placed = (
        P(sp, TP),
        P(sp, TP),
        P(sp, TP),
        P(),
        P(),
        P(None, TP),
        P(sp, TP),
        P(),
        P(sp, None),
        P(sp, None),
        P(sp, None, TP),
        P(sp, None, TP),
        P(sp, None, TP),
    )

    return jax.shard_map(local, mesh=finer, in_specs=placed, out_specs=P(sp, TP), check_vma=False)
```

```python
import jax
import jax.numpy as jnp
from jax import lax
from jax.experimental import pallas as pl
from jax.experimental.pallas import tpu as pltpu
from jax.sharding import Mesh
from jax.sharding import PartitionSpec as P

TP = ("ty", "tx")
NORM_EPS = 1e-06
F32 = jnp.float32
BF16 = jnp.bfloat16


def dot(a, b, ca=1, cb=0):
    return lax.dot_general(a, b, (((ca,), (cb,)), ((), ())), preferred_element_type=F32)


def kernel(body, outs, *args, limit=12, dtype=BF16):
    vmem = pl.BlockSpec(memory_space=pltpu.VMEM)
    got = pl.pallas_call(
        body,
        out_shape=tuple(jax.ShapeDtypeStruct(o, dtype) for o in outs),
        in_specs=[vmem for a in args],
        out_specs=tuple(vmem for o in outs),
        compiler_params=pltpu.CompilerParams(vmem_limit_bytes=limit << 20 if limit else None),
    )(*args)
    return got if len(outs) > 1 else got[0]


def iota(shape, dim):
    return lax.broadcasted_iota(jnp.int32, shape, dim)


def to_row(col, width, offset):
    rows = col.shape[0]
    hit = iota((rows, width), 0) == iota((rows, width), 1) + offset
    return jnp.sum(jnp.where(hit, col, jnp.zeros((), col.dtype)), axis=0, keepdims=True)


def to_col(row, rows, offset):
    width = row.shape[1]
    hit = iota((rows, width), 0) == iota((rows, width), 1) + offset
    return jnp.sum(jnp.where(hit, row, jnp.zeros((), row.dtype)), axis=1, keepdims=True)


def slots(pick_ref, cap):
    toks = pick_ref.shape[0]
    e0 = pick_ref[:, 0:1]
    e1 = pick_ref[:, 1:2]
    experts = iota((toks, 128), 1)
    oh0 = (experts == e0).astype(F32)
    oh1 = (experts == e1).astype(F32)
    earlier = (iota((toks, toks), 0) > iota((toks, toks), 1)).astype(F32).astype(BF16)
    count = dot(earlier, (oh0 + oh1).astype(BF16))
    s0 = jnp.sum(count * oh0, axis=1, keepdims=True).astype(jnp.int32)
    s1 = jnp.sum((count + oh0) * oh1, axis=1, keepdims=True).astype(jnp.int32)
    return jnp.where(s0 < cap, e0 * cap + s0, -1), jnp.where(s1 < cap, e1 * cap + s1, -1)


def routing_out(pick, cap):
    toks = pick.shape[0]

    def body(pick_ref, out_ref):
        t0, t1 = slots(pick_ref, cap)
        place = iota((8, toks), 0)
        out_ref[...] = jnp.where(place == 0, to_row(t0, toks, 0), to_row(t1, toks, 0))

    return kernel(body, ((8, toks),), pick, dtype=jnp.int32)


def project(conv_all, out_weight, residual, slot_rows, rows):
    toks, width = residual.shape

    def body(conv_ref, w_ref, res_ref, slot_ref, stream_ref, out_ref):
        stream = (res_ref[...].astype(F32) + dot(conv_ref[...], w_ref[...], 0, 0)).astype(BF16)
        stream_ref[...] = stream
        across = iota((rows, toks), 0)
        hit = jnp.logical_or(across == slot_ref[0:1, :], across == slot_ref[1:2, :])
        out_ref[...] = dot(hit.astype(F32).astype(BF16), stream).astype(BF16)

    outs = ((toks, width), (rows, width))
    return kernel(body, outs, conv_all, out_weight, residual, slot_rows)


def convolve_head(b_gate, c_gate, h_in, docs, taps):
    chans, toks = h_in.shape
    lane = docs.shape[1]
    per = toks // lane

    def body(*refs):
        given, (total_ref, factor_ref, gate_ref), held = refs[:5], refs[5:8], refs[8:13]
        moves = [pltpu.make_async_copy(g, k, refs[13].at[i]) for i, (g, k) in enumerate(zip(given, held))]
        for move in moves:
            move.start()
        for move in moves:
            move.wait()
        b_ref, c_ref, h_ref, docs_ref, taps_ref = held
        gate_ref[...] = b_ref[...].astype(F32)
        sp = lax.axis_index("z") * 2 + lax.axis_index("core")
        tp = lax.axis_index("ty") * lax.axis_size("tx") + lax.axis_index("tx")
        own = jnp.concatenate([docs_ref[pl.ds(sp * per + k, 1), :] for k in range(per)], axis=1)
        prior = docs_ref[pl.ds(jnp.maximum(sp * per - 1, 0), 1), :]
        prior = jnp.where(sp > 0, prior, -1)
        at = iota((1, toks), 1)
        back1 = jnp.where(at == 0, prior[:, lane - 1 :], pltpu.roll(own, 1, 1))
        back2 = jnp.where(at == 1, prior[:, lane - 1 :], pltpu.roll(own, 2, 1))
        back2 = jnp.where(at == 0, prior[:, lane - 2 : lane - 1], back2)
        same1 = (back1 == own).astype(F32)
        same2 = (back2 == own).astype(F32)
        all_taps = taps_ref[...].astype(F32)
        length = all_taps.shape[1]
        first = lax.rem(length - tp * chans, length)
        near = pltpu.roll(jnp.concatenate([all_taps, jnp.zeros((5, length), F32)]), first, 1)
        tap = [to_col(near[k : k + 1, :chans], chans, 0) for k in range(3)]
        product = (c_ref[...].astype(F32) * h_ref[...].astype(F32)).astype(BF16).astype(F32)
        lanes = iota((chans, toks), 1)
        one = jnp.where(lanes >= 1, pltpu.roll(product, 1, 1), 0.0)
        two = jnp.where(lanes >= 2, pltpu.roll(product, 2, 1), 0.0)
        total_ref[...] = tap[0] * product + tap[1] * one * same1 + tap[2] * two * same2
        place = iota((chans, lane), 1)
        factor = jnp.where(place == 0, tap[1] * same1[:, 0:1], tap[2] * same2[:, 0:1])
        factor_ref[...] = jnp.where(place == 2, tap[2] * same2[:, 1:2], factor)

    outs = ((chans, toks), (chans, lane), (chans, toks))
    args = (b_gate, c_gate, h_in, docs, taps)
    vmem = pl.BlockSpec(memory_space=pltpu.VMEM)
    return pl.pallas_call(
        body,
        out_shape=tuple(jax.ShapeDtypeStruct(o, F32) for o in outs),
        in_specs=[pl.BlockSpec(memory_space=pltpu.HBM)] * len(args),
        out_specs=(vmem,) * len(outs),
        scratch_shapes=[*[pltpu.VMEM(a.shape, a.dtype) for a in args], pltpu.SemaphoreType.DMA((len(args),))],
        compiler_params=pltpu.CompilerParams(vmem_limit_bytes=12 << 20),
        name="convolve_head",
    )(*[pltpu.with_memory_space_constraint(a, pltpu.HBM) for a in args])


def convolve(total, factor, gate, edge, copies):
    chans, toks = gate.shape

    def body(total_ref, factor_ref, gate_ref, edge_ref, out_ref):
        before = [edge_ref[:, k : k + 1].astype(F32) for k in range(2)]
        at0, at1, at2 = (factor_ref[:, k : k + 1] for k in range(3))
        lanes = iota((chans, toks), 1)
        whole = total_ref[...]
        whole = whole + jnp.where(lanes == 0, at0 * before[1], 0.0)
        whole = whole + jnp.where(
            lanes == 0, at1 * before[0], jnp.where(lanes == 1, at2 * before[1], 0.0)
        )
        conv = (gate_ref[...] * whole).astype(BF16)
        for k in range(copies):
            out_ref[k] = conv

    return kernel(body, ((copies, chans, toks),), total, factor, gate, edge)


def order_map(cap, block, splitting):
    q = iota((block, 1), 0)
    if splitting:
        core = (q >= block // 2).astype(jnp.int32)
        within = q - core * (block // 2)
        z = (within * (65536 // cap + 1)) >> 16
        source = within + z * cap + core * cap
    else:
        z = (q * (65536 // (2 * cap) + 1)) >> 16
        rest = q - z * (2 * cap)
        core = (rest >= cap).astype(jnp.int32)
        source = core * (block // 2) + z * cap + rest - core * cap
    return (iota((block, block), 1) == source).astype(F32).astype(BF16)


def split_rows(got, n_tx, cap):
    rows, width = got.shape
    half = rows // 2
    block = 8 * cap
    part = block // 2

    def body(got_ref, out_ref):
        order = order_map(cap, block, True)
        for i in range(rows // block):
            both = dot(order, got_ref[i * block : (i + 1) * block]).astype(BF16)
            for core in range(2):
                for t in range(n_tx):
                    out_ref[core * n_tx + t, i * part : (i + 1) * part] = both[
                        core * part : (core + 1) * part
                    ]

    return kernel(body, ((2 * n_tx, half, width),), got)


def pack(w_gate, w_up, n_ty, steps):
    dim, hid = w_gate.shape
    feats = dim // n_ty

    def body(wg_ref, wu_ref, *rest):
        out_refs, sems = rest[:-1], rest[-1]
        ty = lax.axis_index("ty")
        moves = []
        for k, d in enumerate(steps):
            to = lax.rem(ty + d, n_ty)
            rows = pl.ds(pl.multiple_of(to * feats, feats), feats)
            for j, w_ref in enumerate((wg_ref, wu_ref)):
                lanes = pl.ds(j * hid, hid)
                moves.append(
                    pltpu.make_async_copy(
                        w_ref.at[rows, :], out_refs[k].at[:, lanes], sems.at[2 * k + j]
                    )
                )
        for move in moves:
            move.start()
        for move in moves:
            move.wait()

    return pl.pallas_call(
        body,
        out_shape=tuple(jax.ShapeDtypeStruct((feats, 2 * hid), BF16) for d in steps),
        in_specs=[pl.BlockSpec(memory_space=pltpu.HBM)] * 2,
        out_specs=tuple(pl.BlockSpec(memory_space=pltpu.VMEM) for d in steps),
        scratch_shapes=[pltpu.SemaphoreType.DMA((2 * len(steps),))],
        compiler_params=pltpu.CompilerParams(vmem_limit_bytes=12 << 20),
    )(*[pltpu.with_memory_space_constraint(w, pltpu.HBM) for w in (w_gate, w_up)])


def gate_up(x, gain, w_gate, w_up, pieces):
    n_ty = len(pieces) + 1
    groups, half, width = x.shape
    n_tx = groups // 2
    feats = n_tx * width
    hid = w_gate.shape[1]
    rows = 2 * half

    def body(x_ref, gain_ref, wg_ref, wu_ref, *rest):
        piece_refs, out_ref, held, sems = rest[: n_ty - 1], rest[-3], rest[-2], rest[-1]
        moves = [
            pltpu.make_async_copy(ref, held.at[d], sems.at[d]) for d, ref in enumerate(piece_refs)
        ]
        for move in moves:
            move.start()
        ty = lax.axis_index("ty")
        mine = pl.ds(pl.multiple_of(ty * feats, feats), feats)
        gain_rows = gain_ref[pl.ds(pl.multiple_of(ty * (feats // 128), 8), feats // 128), :].astype(F32)
        gain_row = jnp.concatenate([gain_rows[k : k + 1] for k in range(feats // 128)], axis=1)
        extra = jnp.zeros((8, 2 * hid), F32)
        place = iota((8, 2 * hid), 0)
        scaled = []
        for core in range(2):
            raw = jnp.concatenate([x_ref[core * n_tx + t] for t in range(n_tx)], axis=1).astype(F32)
            squares = jnp.sum(raw * raw, axis=1, keepdims=True)
            y = (raw * gain_row).astype(BF16)
            for k in range(2):
                row = to_row(squares, 2 * hid, k * 2 * hid)
                high = row.astype(BF16).astype(F32)
                at = core * 2 + k
                extra = jnp.where(place == at, high, extra)
                extra = jnp.where(place == at + 4, row - high, extra)
            keep = slice(core * half, (core + 1) * half)
            own = jnp.concatenate([wg_ref[mine, :], wu_ref[mine, :]], axis=1)
            out_ref[ty, keep, :] = dot(y, own).astype(BF16)
            scaled.append(y)
        for d in range(1, n_ty):
            to = lax.rem(ty + (n_ty - d), n_ty)
            moves[d - 1].wait()
            for core in range(2):
                keep = slice(core * half, (core + 1) * half)
                out_ref[to, keep, :] = dot(scaled[core], held[d - 1]).astype(BF16)
        for to in range(n_ty):
            out_ref[to, rows : rows + 8, :] = extra.astype(BF16)

    vmem = pl.BlockSpec(memory_space=pltpu.VMEM)
    anywhere = pl.BlockSpec(memory_space=pltpu.HBM)
    return pl.pallas_call(
        body,
        out_shape=jax.ShapeDtypeStruct((n_ty, rows + 8, 2 * hid), BF16),
        in_specs=[vmem] * 4 + [anywhere] * (n_ty - 1),
        out_specs=vmem,
        scratch_shapes=[
            pltpu.VMEM((n_ty - 1, feats, 2 * hid), BF16),
            pltpu.SemaphoreType.DMA((n_ty - 1,)),
        ],
        compiler_params=pltpu.CompilerParams(vmem_limit_bytes=24 << 20),
        name="gate_up",
    )(x, gain, w_gate, w_up, *[pltpu.with_memory_space_constraint(p, pltpu.HBM) for p in pieces])


def activate(parts, full_dim):
    n_ty, padded, both = parts.shape
    rows, hid = padded - 8, both // 2
    half = rows // 2

    def body(p_ref, out_ref):
        extra = sum(p_ref[k, rows : rows + 8, :].astype(F32) for k in range(n_ty))
        for core in range(2):
            keep = slice(core * half, (core + 1) * half)
            total = sum(p_ref[k, keep, :].astype(F32) for k in range(n_ty))
            squares = jnp.zeros((half, 1), F32)
            for k in range(2):
                at = core * 2 + k
                row = extra[at : at + 1] + extra[at + 4 : at + 5]
                squares = squares + to_col(row, half, k * both)
            total = total * lax.rsqrt(squares / full_dim + NORM_EPS)
            gate, up = total[:, :hid], total[:, hid:]
            hidden = (gate / (1.0 + jnp.exp(-gate)) * up).astype(BF16)
            for k in range(n_ty):
                out_ref[k, keep, :] = hidden

    return kernel(body, ((n_ty, rows, hid),), parts)


def down(hidden, w_down, pieces):
    n_ty, rows, _ = hidden.shape
    n_tx = len(pieces) + 1
    half = rows // 2
    width = w_down.shape[-1]

    def body(h_ref, wd_ref, *rest):
        piece_refs, out_ref = rest[:-1], rest[-1]
        tx = lax.axis_index("tx")
        h = jnp.concatenate([h_ref[k] for k in range(n_ty)], axis=1)
        for d in range(n_tx):
            w = [wd_ref[b, tx] if d == 0 else piece_refs[d - 1][b] for b in range(n_ty)]
            part = dot(h, jnp.concatenate(w, axis=0)).astype(BF16)
            to = lax.rem(tx + (n_tx - d), n_tx)
            out_ref[to] = part[:half]
            out_ref[n_tx + to] = part[half:]

    outs = ((2 * n_tx, half, width),)
    return kernel(body, outs, hidden, w_down, *pieces, limit=24)


def join_rows(parts, cap):
    groups, half, width = parts.shape
    n_tx = groups // 2
    block = 8 * cap
    part = block // 2

    def body(p_ref, out_ref):
        order = order_map(cap, block, False)
        for i in range(2 * half // block):
            keep = slice(i * part, (i + 1) * part)
            both = [
                sum(p_ref[core * n_tx + t, keep].astype(F32) for t in range(n_tx)).astype(BF16)
                for core in range(2)
            ]
            out_ref[i * block : (i + 1) * block] = dot(
                order, jnp.concatenate(both, axis=0)
            ).astype(BF16)

    return kernel(body, ((2 * half, width),), parts)


def combine(back, slot_rows, weights, stream):
    toks = stream.shape[0]
    rows = back.shape[0]

    def body(back_ref, slot_ref, w_ref, stream_ref, out_ref):
        got = back_ref[...]
        lanes = iota((toks, rows), 1)
        total = stream_ref[...].astype(F32)
        feed = jnp.zeros(total.shape, F32)
        for k in range(2):
            slot = to_col(slot_ref[k : k + 1, :], toks, 0)
            picked = dot((lanes == slot).astype(F32).astype(BF16), got)
            feed = feed + picked * to_col(w_ref[k : k + 1, :], toks, 0)
        out_ref[...] = (total + feed).astype(BF16)

    return kernel(body, (stream.shape,), back, slot_rows, weights, stream)


def shifted(value, axis, steps):
    count = lax.axis_size(axis)
    return lax.ppermute(value, axis, [(i, (i + steps) % count) for i in range(count)])


def local(
    b_gate,
    c_gate,
    h_in,
    docs,
    conv_taps,
    out_weight,
    residual_in,
    norm_gain,
    expert_pick,
    route_weight,
    w_gate,
    w_up,
    w_down,
):
    toks, chans = h_in.shape
    width = residual_in.shape[1]
    full_dim = w_gate.shape[1]
    hid = w_gate.shape[2]
    n_z, n_ty, n_tx = (lax.axis_size(a) for a in ("z", "ty", "tx"))
    n_sp = 2 * n_z
    cap = 5 * toks // (2 * n_sp)
    rows = n_sp * cap
    tx = lax.axis_index("tx")

    last = slice(toks - 2, toks)
    product = (c_gate[last].astype(F32) * h_in[last].astype(F32)).astype(BF16)
    edge = lax.ppermute(product, ("z", "core"), [(i, i + 1) for i in range(n_sp - 1)])
    n_tp = n_ty * n_tx
    head = convolve_head(b_gate.T, c_gate.T, h_in.T, docs.reshape(-1, 128), conv_taps)
    conv_copies = convolve(*head, edge.T, n_tp)
    conv_all = lax.all_to_all(conv_copies, TP, 0, 0, tiled=True)
    conv_all = conv_all.reshape(n_tp * chans, toks)

    first = pack(w_gate[0], w_up[0], n_ty, (1, 2))
    (last,) = pack(w_gate[0], w_up[0], n_ty, (3,))
    gate_up_pieces = [shifted(p, "ty", d + 1) for d, p in enumerate(first)]
    gate_up_pieces.append(shifted(last, "ty", 3))
    w_down4 = w_down[0].reshape(n_ty, n_tx, hid, width)
    down_pieces = []
    for d in range(1, n_tx):
        to = lax.rem(tx + d, n_tx)
        piece = lax.dynamic_index_in_dim(w_down4, to, 1, keepdims=False)
        down_pieces.append(shifted(piece, "tx", d))

    slot_rows = routing_out(expert_pick, cap)
    stream, outgoing = project(conv_all, out_weight, residual_in, slot_rows, rows)
    got = lax.all_to_all(
        outgoing.reshape(n_z, 2 * cap, width), "z", 0, 0, tiled=True
    ).reshape(rows, width)
    split = split_rows(got, n_tx, cap)
    x = lax.all_to_all(split, ("core", "tx"), 0, 0, tiled=True)
    parts = gate_up(x, norm_gain.reshape(-1, 128), w_gate[0], w_up[0], gate_up_pieces)
    parts = lax.all_to_all(parts, "ty", 0, 0, tiled=True)
    hidden = activate(parts, full_dim)
    hidden = lax.all_to_all(hidden, "ty", 0, 0, tiled=True)
    outs = lax.all_to_all(
        down(hidden, w_down4, down_pieces), ("core", "tx"), 0, 0, tiled=True
    )
    back = lax.all_to_all(
        join_rows(outs, cap).reshape(n_z, 2 * cap, width), "z", 0, 0, tiled=True
    ).reshape(rows, width)
    return combine(back, slot_rows, route_weight.T, stream)


def solution(mesh):
    finer = Mesh(
        mesh.devices.reshape(mesh.shape["sp"] // 2, 2, 4, 4), ("z", "core", "ty", "tx")
    )
    sp = ("z", "core")
    placed = (
        P(sp, TP),
        P(sp, TP),
        P(sp, TP),
        P(),
        P(),
        P(None, TP),
        P(sp, TP),
        P(),
        P(sp, None),
        P(sp, None),
        P(sp, None, TP),
        P(sp, None, TP),
        P(sp, None, TP),
    )

    return jax.shard_map(local, mesh=finer, in_specs=placed, out_specs=P(sp, TP), check_vma=False)
```

```python
import jax
import jax.numpy as jnp
from jax import lax
from jax.experimental import pallas as pl
from jax.experimental.pallas import tpu as pltpu
from jax.sharding import Mesh
from jax.sharding import PartitionSpec as P

TP = ("ty", "tx")
NORM_EPS = 1e-06
F32 = jnp.float32
BF16 = jnp.bfloat16


def dot(a, b, ca=1, cb=0):
    return lax.dot_general(a, b, (((ca,), (cb,)), ((), ())), preferred_element_type=F32)


def kernel(body, outs, *args, limit=12, dtype=BF16):
    vmem = pl.BlockSpec(memory_space=pltpu.VMEM)
    got = pl.pallas_call(
        body,
        out_shape=tuple(jax.ShapeDtypeStruct(o, dtype) for o in outs),
        in_specs=[vmem for a in args],
        out_specs=tuple(vmem for o in outs),
        compiler_params=pltpu.CompilerParams(vmem_limit_bytes=limit << 20 if limit else None),
    )(*args)
    return got if len(outs) > 1 else got[0]


def iota(shape, dim):
    return lax.broadcasted_iota(jnp.int32, shape, dim)


def to_row(col, width, offset):
    rows = col.shape[0]
    hit = iota((rows, width), 0) == iota((rows, width), 1) + offset
    return jnp.sum(jnp.where(hit, col, jnp.zeros((), col.dtype)), axis=0, keepdims=True)


def to_col(row, rows, offset):
    width = row.shape[1]
    hit = iota((rows, width), 0) == iota((rows, width), 1) + offset
    return jnp.sum(jnp.where(hit, row, jnp.zeros((), row.dtype)), axis=1, keepdims=True)


def slots(pick_ref, cap):
    toks = pick_ref.shape[0]
    e0 = pick_ref[:, 0:1]
    e1 = pick_ref[:, 1:2]
    experts = iota((toks, 128), 1)
    oh0 = (experts == e0).astype(F32)
    oh1 = (experts == e1).astype(F32)
    earlier = (iota((toks, toks), 0) > iota((toks, toks), 1)).astype(F32).astype(BF16)
    count = dot(earlier, (oh0 + oh1).astype(BF16))
    s0 = jnp.sum(count * oh0, axis=1, keepdims=True).astype(jnp.int32)
    s1 = jnp.sum((count + oh0) * oh1, axis=1, keepdims=True).astype(jnp.int32)
    return jnp.where(s0 < cap, e0 * cap + s0, -1), jnp.where(s1 < cap, e1 * cap + s1, -1)


def routing_out(pick, cap):
    toks = pick.shape[0]

    def body(pick_ref, out_ref):
        t0, t1 = slots(pick_ref, cap)
        place = iota((8, toks), 0)
        out_ref[...] = jnp.where(place == 0, to_row(t0, toks, 0), to_row(t1, toks, 0))

    return kernel(body, ((8, toks),), pick, dtype=jnp.int32)


def project(conv_all, out_weight, residual, slot_rows, rows):
    toks, width = residual.shape

    def body(conv_ref, w_ref, res_ref, slot_ref, stream_ref, out_ref):
        stream = (res_ref[...].astype(F32) + dot(conv_ref[...], w_ref[...], 0, 0)).astype(BF16)
        stream_ref[...] = stream
        across = iota((rows, toks), 0)
        hit = jnp.logical_or(across == slot_ref[0:1, :], across == slot_ref[1:2, :])
        out_ref[...] = dot(hit.astype(F32).astype(BF16), stream).astype(BF16)

    outs = ((toks, width), (rows, width))
    return kernel(body, outs, conv_all, out_weight, residual, slot_rows)


def convolve_head(b_gate, c_gate, h_in, docs, taps):
    chans, toks = h_in.shape
    lane = docs.shape[1]
    per = toks // lane

    def body(*refs):
        given, (total_ref, factor_ref, gate_ref), held = refs[:5], refs[5:8], refs[8:13]
        moves = [pltpu.make_async_copy(g, k, refs[13].at[i]) for i, (g, k) in enumerate(zip(given, held))]
        for move in moves:
            move.start()
        for move in moves:
            move.wait()
        b_ref, c_ref, h_ref, docs_ref, taps_ref = held
        gate_ref[...] = b_ref[...].astype(F32)
        sp = lax.axis_index("z") * 2 + lax.axis_index("core")
        tp = lax.axis_index("ty") * lax.axis_size("tx") + lax.axis_index("tx")
        own = jnp.concatenate([docs_ref[pl.ds(sp * per + k, 1), :] for k in range(per)], axis=1)
        prior = docs_ref[pl.ds(jnp.maximum(sp * per - 1, 0), 1), :]
        prior = jnp.where(sp > 0, prior, -1)
        at = iota((1, toks), 1)
        back1 = jnp.where(at == 0, prior[:, lane - 1 :], pltpu.roll(own, 1, 1))
        back2 = jnp.where(at == 1, prior[:, lane - 1 :], pltpu.roll(own, 2, 1))
        back2 = jnp.where(at == 0, prior[:, lane - 2 : lane - 1], back2)
        same1 = (back1 == own).astype(F32)
        same2 = (back2 == own).astype(F32)
        all_taps = taps_ref[...].astype(F32)
        length = all_taps.shape[1]
        first = lax.rem(length - tp * chans, length)
        near = pltpu.roll(jnp.concatenate([all_taps, jnp.zeros((5, length), F32)]), first, 1)
        tap = [to_col(near[k : k + 1, :chans], chans, 0) for k in range(3)]
        product = (c_ref[...].astype(F32) * h_ref[...].astype(F32)).astype(BF16).astype(F32)
        lanes = iota((chans, toks), 1)
        one = jnp.where(lanes >= 1, pltpu.roll(product, 1, 1), 0.0)
        two = jnp.where(lanes >= 2, pltpu.roll(product, 2, 1), 0.0)
        total_ref[...] = tap[0] * product + tap[1] * one * same1 + tap[2] * two * same2
        place = iota((chans, lane), 1)
        factor = jnp.where(place == 0, tap[1] * same1[:, 0:1], tap[2] * same2[:, 0:1])
        factor_ref[...] = jnp.where(place == 2, tap[2] * same2[:, 1:2], factor)

    outs = ((chans, toks), (chans, lane), (chans, toks))
    args = (b_gate, c_gate, h_in, docs, taps)
    vmem = pl.BlockSpec(memory_space=pltpu.VMEM)
    return pl.pallas_call(
        body,
        out_shape=tuple(jax.ShapeDtypeStruct(o, F32) for o in outs),
        in_specs=[pl.BlockSpec(memory_space=pltpu.HBM)] * len(args),
        out_specs=(vmem,) * len(outs),
        scratch_shapes=[*[pltpu.VMEM(a.shape, a.dtype) for a in args], pltpu.SemaphoreType.DMA((len(args),))],
        compiler_params=pltpu.CompilerParams(vmem_limit_bytes=12 << 20),
        name="convolve_head",
    )(*[pltpu.with_memory_space_constraint(a, pltpu.HBM) for a in args])


def convolve(total, factor, gate, edge, copies):
    chans, toks = gate.shape

    def body(total_ref, factor_ref, gate_ref, edge_ref, out_ref):
        before = [edge_ref[:, k : k + 1].astype(F32) for k in range(2)]
        at0, at1, at2 = (factor_ref[:, k : k + 1] for k in range(3))
        lanes = iota((chans, toks), 1)
        whole = total_ref[...]
        whole = whole + jnp.where(lanes == 0, at0 * before[1], 0.0)
        whole = whole + jnp.where(
            lanes == 0, at1 * before[0], jnp.where(lanes == 1, at2 * before[1], 0.0)
        )
        conv = (gate_ref[...] * whole).astype(BF16)
        for k in range(copies):
            out_ref[k] = conv

    return kernel(body, ((copies, chans, toks),), total, factor, gate, edge)


def order_map(cap, block, splitting):
    q = iota((block, 1), 0)
    if splitting:
        core = (q >= block // 2).astype(jnp.int32)
        within = q - core * (block // 2)
        z = (within * (65536 // cap + 1)) >> 16
        source = within + z * cap + core * cap
    else:
        z = (q * (65536 // (2 * cap) + 1)) >> 16
        rest = q - z * (2 * cap)
        core = (rest >= cap).astype(jnp.int32)
        source = core * (block // 2) + z * cap + rest - core * cap
    return (iota((block, block), 1) == source).astype(F32).astype(BF16)


def split_rows(got, n_tx, cap):
    rows, width = got.shape
    half = rows // 2
    block = 8 * cap
    part = block // 2

    def body(got_ref, out_ref):
        order = order_map(cap, block, True)
        for i in range(rows // block):
            both = dot(order, got_ref[i * block : (i + 1) * block]).astype(BF16)
            for core in range(2):
                for t in range(n_tx):
                    out_ref[core * n_tx + t, i * part : (i + 1) * part] = both[
                        core * part : (core + 1) * part
                    ]

    return kernel(body, ((2 * n_tx, half, width),), got)


def pack(w_gate, w_up, n_ty, steps):
    dim, hid = w_gate.shape
    feats = dim // n_ty

    def body(wg_ref, wu_ref, *rest):
        out_refs, sems = rest[:-1], rest[-1]
        ty = lax.axis_index("ty")
        moves = []
        for k, d in enumerate(steps):
            to = lax.rem(ty + d, n_ty)
            rows = pl.ds(pl.multiple_of(to * feats, feats), feats)
            for j, w_ref in enumerate((wg_ref, wu_ref)):
                lanes = pl.ds(j * hid, hid)
                moves.append(
                    pltpu.make_async_copy(
                        w_ref.at[rows, :], out_refs[k].at[:, lanes], sems.at[2 * k + j]
                    )
                )
        for move in moves:
            move.start()
        for move in moves:
            move.wait()

    return pl.pallas_call(
        body,
        out_shape=tuple(jax.ShapeDtypeStruct((feats, 2 * hid), BF16) for d in steps),
        in_specs=[pl.BlockSpec(memory_space=pltpu.HBM)] * 2,
        out_specs=tuple(pl.BlockSpec(memory_space=pltpu.VMEM) for d in steps),
        scratch_shapes=[pltpu.SemaphoreType.DMA((2 * len(steps),))],
        compiler_params=pltpu.CompilerParams(vmem_limit_bytes=12 << 20),
    )(*[pltpu.with_memory_space_constraint(w, pltpu.HBM) for w in (w_gate, w_up)])


def gate_up(x, gain, w_gate, w_up, pieces):
    n_ty = len(pieces) + 1
    groups, half, width = x.shape
    n_tx = groups // 2
    feats = n_tx * width
    hid = w_gate.shape[1]
    rows = 2 * half

    def body(x_ref, gain_ref, wg_ref, wu_ref, *rest):
        piece_refs, out_ref, held, sems = rest[: n_ty - 1], rest[-3], rest[-2], rest[-1]
        moves = [
            pltpu.make_async_copy(ref, held.at[d], sems.at[d]) for d, ref in enumerate(piece_refs)
        ]
        for move in moves:
            move.start()
        ty = lax.axis_index("ty")
        mine = pl.ds(pl.multiple_of(ty * feats, feats), feats)
        gain_rows = gain_ref[pl.ds(pl.multiple_of(ty * (feats // 128), 8), feats // 128), :].astype(F32)
        gain_row = jnp.concatenate([gain_rows[k : k + 1] for k in range(feats // 128)], axis=1)
        extra = jnp.zeros((8, 2 * hid), F32)
        place = iota((8, 2 * hid), 0)
        scaled = []
        for core in range(2):
            raw = jnp.concatenate([x_ref[core * n_tx + t] for t in range(n_tx)], axis=1).astype(F32)
            squares = jnp.sum(raw * raw, axis=1, keepdims=True)
            y = (raw * gain_row).astype(BF16)
            for k in range(2):
                row = to_row(squares, 2 * hid, k * 2 * hid)
                high = row.astype(BF16).astype(F32)
                at = core * 2 + k
                extra = jnp.where(place == at, high, extra)
                extra = jnp.where(place == at + 4, row - high, extra)
            keep = slice(core * half, (core + 1) * half)
            own = jnp.concatenate([wg_ref[mine, :], wu_ref[mine, :]], axis=1)
            out_ref[ty, keep, :] = dot(y, own).astype(BF16)
            scaled.append(y)
        for d in range(1, n_ty):
            to = lax.rem(ty + (n_ty - d), n_ty)
            moves[d - 1].wait()
            for core in range(2):
                keep = slice(core * half, (core + 1) * half)
                out_ref[to, keep, :] = dot(scaled[core], held[d - 1]).astype(BF16)
        for to in range(n_ty):
            out_ref[to, rows : rows + 8, :] = extra.astype(BF16)

    vmem = pl.BlockSpec(memory_space=pltpu.VMEM)
    anywhere = pl.BlockSpec(memory_space=pltpu.HBM)
    return pl.pallas_call(
        body,
        out_shape=jax.ShapeDtypeStruct((n_ty, rows + 8, 2 * hid), BF16),
        in_specs=[vmem] * 4 + [anywhere] * (n_ty - 1),
        out_specs=vmem,
        scratch_shapes=[
            pltpu.VMEM((n_ty - 1, feats, 2 * hid), BF16),
            pltpu.SemaphoreType.DMA((n_ty - 1,)),
        ],
        compiler_params=pltpu.CompilerParams(vmem_limit_bytes=24 << 20),
        name="gate_up",
    )(x, gain, w_gate, w_up, *[pltpu.with_memory_space_constraint(p, pltpu.HBM) for p in pieces])


def activate(parts, full_dim):
    n_ty, padded, both = parts.shape
    rows, hid = padded - 8, both // 2
    half = rows // 2

    def body(p_ref, out_ref):
        extra = sum(p_ref[k, rows : rows + 8, :].astype(F32) for k in range(n_ty))
        for core in range(2):
            keep = slice(core * half, (core + 1) * half)
            total = sum(p_ref[k, keep, :].astype(F32) for k in range(n_ty))
            squares = jnp.zeros((half, 1), F32)
            for k in range(2):
                at = core * 2 + k
                row = extra[at : at + 1] + extra[at + 4 : at + 5]
                squares = squares + to_col(row, half, k * both)
            total = total * lax.rsqrt(squares / full_dim + NORM_EPS)
            gate, up = total[:, :hid], total[:, hid:]
            hidden = (gate / (1.0 + jnp.exp(-gate)) * up).astype(BF16)
            for k in range(n_ty):
                out_ref[k, keep, :] = hidden

    return kernel(body, ((n_ty, rows, hid),), parts)


def down(hidden, w_down, pieces):
    n_ty, rows, _ = hidden.shape
    n_tx = len(pieces) + 1
    half = rows // 2
    width = w_down.shape[-1]

    def body(h_ref, wd_ref, *rest):
        piece_refs, out_ref = rest[:-1], rest[-1]
        tx = lax.axis_index("tx")
        h = jnp.concatenate([h_ref[k] for k in range(n_ty)], axis=1)
        for d in range(n_tx):
            w = [wd_ref[b, tx] if d == 0 else piece_refs[d - 1][b] for b in range(n_ty)]
            part = dot(h, jnp.concatenate(w, axis=0)).astype(BF16)
            to = lax.rem(tx + (n_tx - d), n_tx)
            out_ref[to] = part[:half]
            out_ref[n_tx + to] = part[half:]

    outs = ((2 * n_tx, half, width),)
    return kernel(body, outs, hidden, w_down, *pieces, limit=24)


def stage(pieces):
    count = len(pieces)

    def body(*refs):
        moves = [
            pltpu.make_async_copy(refs[d], refs[count + d], refs[-1].at[d]) for d in range(count)
        ]
        for move in moves:
            move.start()
        for move in moves:
            move.wait()

    return pl.pallas_call(
        body,
        out_shape=tuple(jax.ShapeDtypeStruct(p.shape, p.dtype) for p in pieces),
        in_specs=[pl.BlockSpec(memory_space=pltpu.HBM)] * count,
        out_specs=tuple(pl.BlockSpec(memory_space=pltpu.VMEM) for p in pieces),
        scratch_shapes=[pltpu.SemaphoreType.DMA((count,))],
        compiler_params=pltpu.CompilerParams(vmem_limit_bytes=12 << 20),
        name="stage",
    )(*[pltpu.with_memory_space_constraint(p, pltpu.HBM) for p in pieces])


def join_rows(parts, cap):
    groups, half, width = parts.shape
    n_tx = groups // 2
    block = 8 * cap
    part = block // 2

    def body(p_ref, out_ref):
        order = order_map(cap, block, False)
        for i in range(2 * half // block):
            keep = slice(i * part, (i + 1) * part)
            both = [
                sum(p_ref[core * n_tx + t, keep].astype(F32) for t in range(n_tx)).astype(BF16)
                for core in range(2)
            ]
            out_ref[i * block : (i + 1) * block] = dot(
                order, jnp.concatenate(both, axis=0)
            ).astype(BF16)

    return kernel(body, ((2 * half, width),), parts)


def combine(back, slot_rows, weights, stream):
    toks = stream.shape[0]
    rows = back.shape[0]

    def body(back_ref, slot_ref, w_ref, stream_ref, out_ref):
        got = back_ref[...]
        lanes = iota((toks, rows), 1)
        total = stream_ref[...].astype(F32)
        feed = jnp.zeros(total.shape, F32)
        for k in range(2):
            slot = to_col(slot_ref[k : k + 1, :], toks, 0)
            picked = dot((lanes == slot).astype(F32).astype(BF16), got)
            feed = feed + picked * to_col(w_ref[k : k + 1, :], toks, 0)
        out_ref[...] = (total + feed).astype(BF16)

    return kernel(body, (stream.shape,), back, slot_rows, weights, stream)


def shifted(value, axis, steps):
    count = lax.axis_size(axis)
    return lax.ppermute(value, axis, [(i, (i + steps) % count) for i in range(count)])


def local(
    b_gate,
    c_gate,
    h_in,
    docs,
    conv_taps,
    out_weight,
    residual_in,
    norm_gain,
    expert_pick,
    route_weight,
    w_gate,
    w_up,
    w_down,
):
    toks, chans = h_in.shape
    width = residual_in.shape[1]
    full_dim = w_gate.shape[1]
    hid = w_gate.shape[2]
    n_z, n_ty, n_tx = (lax.axis_size(a) for a in ("z", "ty", "tx"))
    n_sp = 2 * n_z
    cap = 5 * toks // (2 * n_sp)
    rows = n_sp * cap
    tx = lax.axis_index("tx")

    last = slice(toks - 2, toks)
    product = (c_gate[last].astype(F32) * h_in[last].astype(F32)).astype(BF16)
    edge = lax.ppermute(product, ("z", "core"), [(i, i + 1) for i in range(n_sp - 1)])
    n_tp = n_ty * n_tx
    head = convolve_head(b_gate.T, c_gate.T, h_in.T, docs.reshape(-1, 128), conv_taps)
    conv_copies = convolve(*head, edge.T, n_tp)
    conv_all = lax.all_to_all(conv_copies, TP, 0, 0, tiled=True)
    conv_all = conv_all.reshape(n_tp * chans, toks)

    first = pack(w_gate[0], w_up[0], n_ty, (1, 2))
    (last,) = pack(w_gate[0], w_up[0], n_ty, (3,))
    gate_up_pieces = [shifted(p, "ty", d + 1) for d, p in enumerate(first)]
    gate_up_pieces.append(shifted(last, "ty", 3))
    w_down4 = w_down[0].reshape(n_ty, n_tx, hid, width)
    down_pieces = []
    for d in range(1, n_tx):
        to = lax.rem(tx + d, n_tx)
        piece = lax.dynamic_index_in_dim(w_down4, to, 1, keepdims=False)
        down_pieces.append(shifted(piece, "tx", d))

    slot_rows = routing_out(expert_pick, cap)
    stream, outgoing = project(conv_all, out_weight, residual_in, slot_rows, rows)
    got = lax.all_to_all(
        outgoing.reshape(n_z, 2 * cap, width), "z", 0, 0, tiled=True
    ).reshape(rows, width)
    split = split_rows(got, n_tx, cap)
    x = lax.all_to_all(split, ("core", "tx"), 0, 0, tiled=True)
    parts = gate_up(x, norm_gain.reshape(-1, 128), w_gate[0], w_up[0], gate_up_pieces)
    parts = lax.all_to_all(parts, "ty", 0, 0, tiled=True)
    hidden = activate(parts, full_dim)
    hidden = lax.all_to_all(hidden, "ty", 0, 0, tiled=True)
    outs = lax.all_to_all(
        down(hidden, w_down4, stage(down_pieces)), ("core", "tx"), 0, 0, tiled=True
    )
    back = lax.all_to_all(
        join_rows(outs, cap).reshape(n_z, 2 * cap, width), "z", 0, 0, tiled=True
    ).reshape(rows, width)
    return combine(back, slot_rows, route_weight.T, stream)


def solution(mesh):
    finer = Mesh(
        mesh.devices.reshape(mesh.shape["sp"] // 2, 2, 4, 4), ("z", "core", "ty", "tx")
    )
    sp = ("z", "core")
    placed = (
        P(sp, TP),
        P(sp, TP),
        P(sp, TP),
        P(),
        P(),
        P(None, TP),
        P(sp, TP),
        P(),
        P(sp, None),
        P(sp, None),
        P(sp, None, TP),
        P(sp, None, TP),
        P(sp, None, TP),
    )

    return jax.shard_map(local, mesh=finer, in_specs=placed, out_specs=P(sp, TP), check_vma=False)
```

```python
import jax
import jax.numpy as jnp
from jax import lax
from jax.experimental import pallas as pl
from jax.experimental.pallas import tpu as pltpu
from jax.sharding import Mesh
from jax.sharding import PartitionSpec as P

TP = ("ty", "tx")
NORM_EPS = 1e-06
F32 = jnp.float32
BF16 = jnp.bfloat16


def dot(a, b, ca=1, cb=0):
    return lax.dot_general(a, b, (((ca,), (cb,)), ((), ())), preferred_element_type=F32)


def kernel(body, outs, *args, limit=12, dtype=BF16):
    vmem = pl.BlockSpec(memory_space=pltpu.VMEM)
    got = pl.pallas_call(
        body,
        out_shape=tuple(jax.ShapeDtypeStruct(o, dtype) for o in outs),
        in_specs=[vmem for a in args],
        out_specs=tuple(vmem for o in outs),
        compiler_params=pltpu.CompilerParams(vmem_limit_bytes=limit << 20 if limit else None),
    )(*args)
    return got if len(outs) > 1 else got[0]


def iota(shape, dim):
    return lax.broadcasted_iota(jnp.int32, shape, dim)


def to_row(col, width, offset):
    rows = col.shape[0]
    hit = iota((rows, width), 0) == iota((rows, width), 1) + offset
    return jnp.sum(jnp.where(hit, col, jnp.zeros((), col.dtype)), axis=0, keepdims=True)


def to_col(row, rows, offset):
    width = row.shape[1]
    hit = iota((rows, width), 0) == iota((rows, width), 1) + offset
    return jnp.sum(jnp.where(hit, row, jnp.zeros((), row.dtype)), axis=1, keepdims=True)


def slots(pick_ref, cap):
    toks = pick_ref.shape[0]
    e0 = pick_ref[:, 0:1]
    e1 = pick_ref[:, 1:2]
    experts = iota((toks, 128), 1)
    oh0 = (experts == e0).astype(F32)
    oh1 = (experts == e1).astype(F32)
    earlier = (iota((toks, toks), 0) > iota((toks, toks), 1)).astype(F32).astype(BF16)
    count = dot(earlier, (oh0 + oh1).astype(BF16))
    s0 = jnp.sum(count * oh0, axis=1, keepdims=True).astype(jnp.int32)
    s1 = jnp.sum((count + oh0) * oh1, axis=1, keepdims=True).astype(jnp.int32)
    return jnp.where(s0 < cap, e0 * cap + s0, -1), jnp.where(s1 < cap, e1 * cap + s1, -1)


def routing_out(pick, cap):
    toks = pick.shape[0]

    def body(pick_ref, out_ref):
        t0, t1 = slots(pick_ref, cap)
        place = iota((8, toks), 0)
        out_ref[...] = jnp.where(place == 0, to_row(t0, toks, 0), to_row(t1, toks, 0))

    return kernel(body, ((8, toks),), pick, dtype=jnp.int32)


def project(conv_all, out_weight, residual, slot_rows, rows):
    toks, width = residual.shape

    def body(conv_ref, w_ref, res_ref, slot_ref, stream_ref, out_ref):
        stream = (res_ref[...].astype(F32) + dot(conv_ref[...], w_ref[...], 0, 0)).astype(BF16)
        stream_ref[...] = stream
        across = iota((rows, toks), 0)
        hit = jnp.logical_or(across == slot_ref[0:1, :], across == slot_ref[1:2, :])
        out_ref[...] = dot(hit.astype(F32).astype(BF16), stream).astype(BF16)

    outs = ((toks, width), (rows, width))
    return kernel(body, outs, conv_all, out_weight, residual, slot_rows)


def convolve_head(b_gate, c_gate, h_in, docs, taps):
    chans, toks = h_in.shape
    lane = docs.shape[1]
    per = toks // lane

    def body(*refs):
        given, (total_ref, factor_ref, gate_ref), held = refs[:5], refs[5:8], refs[8:13]
        moves = [pltpu.make_async_copy(g, k, refs[13].at[i]) for i, (g, k) in enumerate(zip(given, held))]
        for move in moves:
            move.start()
        for move in moves:
            move.wait()
        b_ref, c_ref, h_ref, docs_ref, taps_ref = held
        gate_ref[...] = b_ref[...].astype(F32)
        sp = lax.axis_index("z") * 2 + lax.axis_index("core")
        tp = lax.axis_index("ty") * lax.axis_size("tx") + lax.axis_index("tx")
        own = jnp.concatenate([docs_ref[pl.ds(sp * per + k, 1), :] for k in range(per)], axis=1)
        prior = docs_ref[pl.ds(jnp.maximum(sp * per - 1, 0), 1), :]
        prior = jnp.where(sp > 0, prior, -1)
        at = iota((1, toks), 1)
        back1 = jnp.where(at == 0, prior[:, lane - 1 :], pltpu.roll(own, 1, 1))
        back2 = jnp.where(at == 1, prior[:, lane - 1 :], pltpu.roll(own, 2, 1))
        back2 = jnp.where(at == 0, prior[:, lane - 2 : lane - 1], back2)
        same1 = (back1 == own).astype(F32)
        same2 = (back2 == own).astype(F32)
        all_taps = taps_ref[...].astype(F32)
        length = all_taps.shape[1]
        first = lax.rem(length - tp * chans, length)
        near = pltpu.roll(jnp.concatenate([all_taps, jnp.zeros((5, length), F32)]), first, 1)
        tap = [to_col(near[k : k + 1, :chans], chans, 0) for k in range(3)]
        product = (c_ref[...].astype(F32) * h_ref[...].astype(F32)).astype(BF16).astype(F32)
        lanes = iota((chans, toks), 1)
        one = jnp.where(lanes >= 1, pltpu.roll(product, 1, 1), 0.0)
        two = jnp.where(lanes >= 2, pltpu.roll(product, 2, 1), 0.0)
        total_ref[...] = tap[0] * product + tap[1] * one * same1 + tap[2] * two * same2
        place = iota((chans, lane), 1)
        factor = jnp.where(place == 0, tap[1] * same1[:, 0:1], tap[2] * same2[:, 0:1])
        factor_ref[...] = jnp.where(place == 2, tap[2] * same2[:, 1:2], factor)

    outs = ((chans, toks), (chans, lane), (chans, toks))
    args = (b_gate, c_gate, h_in, docs, taps)
    vmem = pl.BlockSpec(memory_space=pltpu.VMEM)
    return pl.pallas_call(
        body,
        out_shape=tuple(jax.ShapeDtypeStruct(o, F32) for o in outs),
        in_specs=[pl.BlockSpec(memory_space=pltpu.HBM)] * len(args),
        out_specs=(vmem,) * len(outs),
        scratch_shapes=[*[pltpu.VMEM(a.shape, a.dtype) for a in args], pltpu.SemaphoreType.DMA((len(args),))],
        compiler_params=pltpu.CompilerParams(vmem_limit_bytes=12 << 20),
        name="convolve_head",
    )(*[pltpu.with_memory_space_constraint(a, pltpu.HBM) for a in args])


def convolve(total, factor, gate, edge, copies):
    chans, toks = gate.shape

    def body(total_ref, factor_ref, gate_ref, edge_ref, out_ref):
        before = [edge_ref[:, k : k + 1].astype(F32) for k in range(2)]
        at0, at1, at2 = (factor_ref[:, k : k + 1] for k in range(3))
        lanes = iota((chans, toks), 1)
        whole = total_ref[...]
        whole = whole + jnp.where(lanes == 0, at0 * before[1], 0.0)
        whole = whole + jnp.where(
            lanes == 0, at1 * before[0], jnp.where(lanes == 1, at2 * before[1], 0.0)
        )
        conv = (gate_ref[...] * whole).astype(BF16)
        for k in range(copies):
            out_ref[k] = conv

    return kernel(body, ((copies, chans, toks),), total, factor, gate, edge)


def order_map(cap, block, splitting):
    q = iota((block, 1), 0)
    if splitting:
        core = (q >= block // 2).astype(jnp.int32)
        within = q - core * (block // 2)
        z = (within * (65536 // cap + 1)) >> 16
        source = within + z * cap + core * cap
    else:
        z = (q * (65536 // (2 * cap) + 1)) >> 16
        rest = q - z * (2 * cap)
        core = (rest >= cap).astype(jnp.int32)
        source = core * (block // 2) + z * cap + rest - core * cap
    return (iota((block, block), 1) == source).astype(F32).astype(BF16)


def split_rows(got, n_tx, cap):
    rows, width = got.shape
    half = rows // 2
    block = 8 * cap
    part = block // 2

    def body(got_ref, out_ref):
        order = order_map(cap, block, True)
        for i in range(rows // block):
            both = dot(order, got_ref[i * block : (i + 1) * block]).astype(BF16)
            for core in range(2):
                for t in range(n_tx):
                    out_ref[core * n_tx + t, i * part : (i + 1) * part] = both[
                        core * part : (core + 1) * part
                    ]

    return kernel(body, ((2 * n_tx, half, width),), got)


def pack(w_gate, w_up, n_ty, steps):
    dim, hid = w_gate.shape
    feats = dim // n_ty

    def body(wg_ref, wu_ref, *rest):
        count = len(steps)
        out_refs, held, sems = rest[:count], rest[count], rest[count + 1]
        ty = lax.axis_index("ty")
        reads, writes = [], []
        for k, d in enumerate(steps):
            to = lax.rem(ty + d, n_ty)
            rows = pl.ds(pl.multiple_of(to * feats, feats), feats)
            for j, w_ref in enumerate((wg_ref, wu_ref)):
                lanes = pl.ds(j * hid, hid)
                move = pltpu.make_async_copy(
                    w_ref.at[rows, :], held.at[k, :, lanes], sems.at[3 * k + j]
                )
                move.start()
                reads.append(move)
        for k in range(count):
            reads[2 * k].wait()
            reads[2 * k + 1].wait()
            move = pltpu.make_async_copy(held.at[k], out_refs[k], sems.at[3 * k + 2])
            move.start()
            writes.append(move)
        for move in writes:
            move.wait()

    return pl.pallas_call(
        body,
        out_shape=tuple(jax.ShapeDtypeStruct((feats, 2 * hid), BF16) for d in steps),
        in_specs=[pl.BlockSpec(memory_space=pltpu.HBM)] * 2,
        out_specs=tuple(pl.BlockSpec(memory_space=pl.ANY) for d in steps),
        scratch_shapes=[
            pltpu.VMEM((len(steps), feats, 2 * hid), BF16),
            pltpu.SemaphoreType.DMA((3 * len(steps),)),
        ],
        compiler_params=pltpu.CompilerParams(vmem_limit_bytes=12 << 20),
    )(*[pltpu.with_memory_space_constraint(w, pltpu.HBM) for w in (w_gate, w_up)])


def gate_up(x, gain, w_gate, w_up, pieces):
    n_ty = len(pieces) + 1
    groups, half, width = x.shape
    n_tx = groups // 2
    feats = n_tx * width
    hid = w_gate.shape[1]
    rows = 2 * half

    def body(x_ref, gain_ref, wg_ref, wu_ref, *rest):
        piece_refs, out_ref, held, sems = rest[: n_ty - 1], rest[-3], rest[-2], rest[-1]
        moves = [
            pltpu.make_async_copy(ref, held.at[d], sems.at[d]) for d, ref in enumerate(piece_refs)
        ]
        for move in moves:
            move.start()
        ty = lax.axis_index("ty")
        mine = pl.ds(pl.multiple_of(ty * feats, feats), feats)
        gain_rows = gain_ref[pl.ds(pl.multiple_of(ty * (feats // 128), 8), feats // 128), :].astype(F32)
        gain_row = jnp.concatenate([gain_rows[k : k + 1] for k in range(feats // 128)], axis=1)
        extra = jnp.zeros((8, 2 * hid), F32)
        place = iota((8, 2 * hid), 0)
        scaled = []
        for core in range(2):
            raw = jnp.concatenate([x_ref[core * n_tx + t] for t in range(n_tx)], axis=1).astype(F32)
            squares = jnp.sum(raw * raw, axis=1, keepdims=True)
            y = (raw * gain_row).astype(BF16)
            for k in range(2):
                row = to_row(squares, 2 * hid, k * 2 * hid)
                high = row.astype(BF16).astype(F32)
                at = core * 2 + k
                extra = jnp.where(place == at, high, extra)
                extra = jnp.where(place == at + 4, row - high, extra)
            keep = slice(core * half, (core + 1) * half)
            own = jnp.concatenate([wg_ref[mine, :], wu_ref[mine, :]], axis=1)
            out_ref[ty, keep, :] = dot(y, own).astype(BF16)
            scaled.append(y)
        for d in range(1, n_ty):
            to = lax.rem(ty + (n_ty - d), n_ty)
            moves[d - 1].wait()
            for core in range(2):
                keep = slice(core * half, (core + 1) * half)
                out_ref[to, keep, :] = dot(scaled[core], held[d - 1]).astype(BF16)
        for to in range(n_ty):
            out_ref[to, rows : rows + 8, :] = extra.astype(BF16)

    vmem = pl.BlockSpec(memory_space=pltpu.VMEM)
    anywhere = pl.BlockSpec(memory_space=pltpu.HBM)
    return pl.pallas_call(
        body,
        out_shape=jax.ShapeDtypeStruct((n_ty, rows + 8, 2 * hid), BF16),
        in_specs=[vmem] * 4 + [anywhere] * (n_ty - 1),
        out_specs=vmem,
        scratch_shapes=[
            pltpu.VMEM((n_ty - 1, feats, 2 * hid), BF16),
            pltpu.SemaphoreType.DMA((n_ty - 1,)),
        ],
        compiler_params=pltpu.CompilerParams(vmem_limit_bytes=24 << 20),
        name="gate_up",
    )(x, gain, w_gate, w_up, *[pltpu.with_memory_space_constraint(p, pltpu.HBM) for p in pieces])


def activate(parts, full_dim):
    n_ty, padded, both = parts.shape
    rows, hid = padded - 8, both // 2
    half = rows // 2

    def body(p_ref, out_ref):
        extra = sum(p_ref[k, rows : rows + 8, :].astype(F32) for k in range(n_ty))
        for core in range(2):
            keep = slice(core * half, (core + 1) * half)
            total = sum(p_ref[k, keep, :].astype(F32) for k in range(n_ty))
            squares = jnp.zeros((half, 1), F32)
            for k in range(2):
                at = core * 2 + k
                row = extra[at : at + 1] + extra[at + 4 : at + 5]
                squares = squares + to_col(row, half, k * both)
            total = total * lax.rsqrt(squares / full_dim + NORM_EPS)
            gate, up = total[:, :hid], total[:, hid:]
            hidden = (gate / (1.0 + jnp.exp(-gate)) * up).astype(BF16)
            for k in range(n_ty):
                out_ref[k, keep, :] = hidden

    return kernel(body, ((n_ty, rows, hid),), parts)


def down(hidden, w_down, pieces):
    n_ty, rows, _ = hidden.shape
    n_tx = len(pieces) + 1
    half = rows // 2
    width = w_down.shape[-1]

    def body(h_ref, wd_ref, *rest):
        piece_refs, out_ref = rest[:-1], rest[-1]
        tx = lax.axis_index("tx")
        h = jnp.concatenate([h_ref[k] for k in range(n_ty)], axis=1)
        for d in range(n_tx):
            w = [wd_ref[b, tx] if d == 0 else piece_refs[d - 1][b] for b in range(n_ty)]
            part = dot(h, jnp.concatenate(w, axis=0)).astype(BF16)
            to = lax.rem(tx + (n_tx - d), n_tx)
            out_ref[to] = part[:half]
            out_ref[n_tx + to] = part[half:]

    outs = ((2 * n_tx, half, width),)
    return kernel(body, outs, hidden, w_down, *pieces, limit=24)


def stage(pieces):
    count = len(pieces)

    def body(*refs):
        moves = [
            pltpu.make_async_copy(refs[d], refs[count + d], refs[-1].at[d]) for d in range(count)
        ]
        for move in moves:
            move.start()
        for move in moves:
            move.wait()

    return pl.pallas_call(
        body,
        out_shape=tuple(jax.ShapeDtypeStruct(p.shape, p.dtype) for p in pieces),
        in_specs=[pl.BlockSpec(memory_space=pltpu.HBM)] * count,
        out_specs=tuple(pl.BlockSpec(memory_space=pltpu.VMEM) for p in pieces),
        scratch_shapes=[pltpu.SemaphoreType.DMA((count,))],
        compiler_params=pltpu.CompilerParams(vmem_limit_bytes=12 << 20),
        name="stage",
    )(*[pltpu.with_memory_space_constraint(p, pltpu.HBM) for p in pieces])


def join_rows(parts, cap):
    groups, half, width = parts.shape
    n_tx = groups // 2
    block = 8 * cap
    part = block // 2

    def body(p_ref, out_ref):
        order = order_map(cap, block, False)
        for i in range(2 * half // block):
            keep = slice(i * part, (i + 1) * part)
            both = [
                sum(p_ref[core * n_tx + t, keep].astype(F32) for t in range(n_tx)).astype(BF16)
                for core in range(2)
            ]
            out_ref[i * block : (i + 1) * block] = dot(
                order, jnp.concatenate(both, axis=0)
            ).astype(BF16)

    return kernel(body, ((2 * half, width),), parts)


def combine(back, slot_rows, weights, stream):
    toks = stream.shape[0]
    rows = back.shape[0]

    def body(back_ref, slot_ref, w_ref, stream_ref, out_ref):
        got = back_ref[...]
        lanes = iota((toks, rows), 1)
        total = stream_ref[...].astype(F32)
        feed = jnp.zeros(total.shape, F32)
        for k in range(2):
            slot = to_col(slot_ref[k : k + 1, :], toks, 0)
            picked = dot((lanes == slot).astype(F32).astype(BF16), got)
            feed = feed + picked * to_col(w_ref[k : k + 1, :], toks, 0)
        out_ref[...] = (total + feed).astype(BF16)

    return kernel(body, (stream.shape,), back, slot_rows, weights, stream)


def shifted(value, axis, steps):
    count = lax.axis_size(axis)
    return lax.ppermute(value, axis, [(i, (i + steps) % count) for i in range(count)])


def local(
    b_gate,
    c_gate,
    h_in,
    docs,
    conv_taps,
    out_weight,
    residual_in,
    norm_gain,
    expert_pick,
    route_weight,
    w_gate,
    w_up,
    w_down,
):
    toks, chans = h_in.shape
    width = residual_in.shape[1]
    full_dim = w_gate.shape[1]
    hid = w_gate.shape[2]
    n_z, n_ty, n_tx = (lax.axis_size(a) for a in ("z", "ty", "tx"))
    n_sp = 2 * n_z
    cap = 5 * toks // (2 * n_sp)
    rows = n_sp * cap
    tx = lax.axis_index("tx")

    last = slice(toks - 2, toks)
    product = (c_gate[last].astype(F32) * h_in[last].astype(F32)).astype(BF16)
    edge = lax.ppermute(product, ("z", "core"), [(i, i + 1) for i in range(n_sp - 1)])
    n_tp = n_ty * n_tx
    head = convolve_head(b_gate.T, c_gate.T, h_in.T, docs.reshape(-1, 128), conv_taps)
    conv_copies = convolve(*head, edge.T, n_tp)
    conv_all = lax.all_to_all(conv_copies, TP, 0, 0, tiled=True)
    conv_all = conv_all.reshape(n_tp * chans, toks)

    first = pack(w_gate[0], w_up[0], n_ty, (1, 2))
    (last,) = pack(w_gate[0], w_up[0], n_ty, (3,))
    gate_up_pieces = [shifted(p, "ty", d + 1) for d, p in enumerate(first)]
    gate_up_pieces.append(shifted(last, "ty", 3))
    w_down4 = w_down[0].reshape(n_ty, n_tx, hid, width)
    down_pieces = []
    for d in range(1, n_tx):
        to = lax.rem(tx + d, n_tx)
        piece = lax.dynamic_index_in_dim(w_down4, to, 1, keepdims=False)
        down_pieces.append(shifted(piece, "tx", d))

    slot_rows = routing_out(expert_pick, cap)
    stream, outgoing = project(conv_all, out_weight, residual_in, slot_rows, rows)
    got = lax.all_to_all(
        outgoing.reshape(n_z, 2 * cap, width), "z", 0, 0, tiled=True
    ).reshape(rows, width)
    split = split_rows(got, n_tx, cap)
    x = lax.all_to_all(split, ("core", "tx"), 0, 0, tiled=True)
    parts = gate_up(x, norm_gain.reshape(-1, 128), w_gate[0], w_up[0], gate_up_pieces)
    parts = lax.all_to_all(parts, "ty", 0, 0, tiled=True)
    hidden = activate(parts, full_dim)
    hidden = lax.all_to_all(hidden, "ty", 0, 0, tiled=True)
    outs = lax.all_to_all(
        down(hidden, w_down4, stage(down_pieces)), ("core", "tx"), 0, 0, tiled=True
    )
    back = lax.all_to_all(
        join_rows(outs, cap).reshape(n_z, 2 * cap, width), "z", 0, 0, tiled=True
    ).reshape(rows, width)
    return combine(back, slot_rows, route_weight.T, stream)


def solution(mesh):
    finer = Mesh(
        mesh.devices.reshape(mesh.shape["sp"] // 2, 2, 4, 4), ("z", "core", "ty", "tx")
    )
    sp = ("z", "core")
    placed = (
        P(sp, TP),
        P(sp, TP),
        P(sp, TP),
        P(),
        P(),
        P(None, TP),
        P(sp, TP),
        P(),
        P(sp, None),
        P(sp, None),
        P(sp, None, TP),
        P(sp, None, TP),
        P(sp, None, TP),
    )

    return jax.shard_map(local, mesh=finer, in_specs=placed, out_specs=P(sp, TP), check_vma=False)
```
